32 devices in a mesh: ep: 8 (over z, y), tp: 4 (over x, core).
Axes of the slice: x: 2, y: 2, z: 4, core: 2. Of those that a mesh axis runs over, the one named last changes fastest.
Arguments:
- queries: bfloat16 [1024, 512], P('ep', 'tp'), may hold values from -8 to 8
- key_cache: bfloat16 [4, 64, 1024], P('tp', None, 'ep'), may hold values from -4.5 to 4.5
- value_cache: bfloat16 [4, 64, 1024], P('tp', None, 'ep'), may hold values from -6 to 6
- cum_gate: float32 [4, 1024], P('tp'), may hold values from -256 to 0, as said below
- out_weight: bfloat16 [512, 2048], replicated, may hold values from -1 to 1
- routed_input: bfloat16 [2048, 2048], P('ep'), may hold values from -6 to 6
- norm_gain: bfloat16 [2048], replicated, may hold values from 0.099609375 to 1.8984375
- routes: int32 [2048, 2], P('ep'), may hold values from 0 to 7, all different within a row; in each aligned block of 64 rows (0 to 63, 64 to 127, ...) at most 24 rows name the same one
- route_weight: float32 [2048, 2], P('ep'), may hold values from 0.2 to 1
- expert_gate: bfloat16 [8, 2048, 1024], P('ep', None, 'tp'), may hold values from -0.125 to 0.125
- expert_up: bfloat16 [8, 2048, 1024], P('ep', None, 'tp'), may hold values from -0.125 to 0.125
- expert_down: bfloat16 [8, 1024, 2048], P('ep', 'tp'), may hold values from -0.1875 to 0.1875
Outputs:
- mixed_out: bfloat16 [1024, 2048], P(('ep', 'tp'))
- expert_out: bfloat16 [2048, 2048], P(('ep', 'tp'))
The draws below stay inside these ranges and needn't reach their ends.
Inputs may be any that keep to these rules, and one draw needn't show every extreme that they name: `cum_gate`: Non-increasing along positions in every head. `routes`: each row names 2 different experts. In each aligned block of 64 rows (the rows of one device) no expert is named by more than 24 rows, a bound that some block reaches.
All inputs are finite; a program needn't handle non-finite values.
Results may differ from the reference program's by a relative error of at most 0.012.
Values may be sent and summed in bfloat16 or wider, within the bound.
A program may use at most 64 MiB of HBM per device.

```python
import math
import jax
import jax.numpy as jnp
import numpy as np
from jax import lax

D = 2048
HEADS = 8
HEAD = 64
KV_HEADS = 4
FFE = 1024
TOPK = 2
SEQ_ROWS = 128
TOK_DEV = 64
FIRST_TOKENS = 1024
ROUTED_TOKENS = 2048
EXPERTS = 8
CAP = 24
N_TP = 4


def draw_queries(key, part):
    base_key = jax.random.fold_in(key, 11)
    values = jnp.clip(jax.random.normal(base_key, (FIRST_TOKENS, HEADS * HEAD), jnp.float32), -4.0, 4.0)
    return values.astype(jnp.bfloat16)


def draw_key_cache(key, part):
    base_key = jax.random.fold_in(key, 13)
    values = jnp.clip(jax.random.normal(base_key, (KV_HEADS, HEAD, FIRST_TOKENS), jnp.float32), -4.0, 4.0)
    return values.astype(jnp.bfloat16)


def draw_cum_gate(key, part):
    ordering_random_key, gradual_random_key, quick_random_key, block_random_key, coarse_random_key, spike_random_key, loss_random_key = jax.random.split(jax.random.fold_in(key, 17), 7)
    ranks = jax.random.permutation(ordering_random_key, KV_HEADS)
    gradual_decay = ranks < KV_HEADS // 2
    rough = jax.random.uniform(coarse_random_key, (KV_HEADS, FIRST_TOKENS), jnp.float32, 0.2, 1.8)
    slow_rate = jax.random.uniform(gradual_random_key, (KV_HEADS,), jnp.float32, 0.1, 0.4) / FIRST_TOKENS
    fast_rate = 1.0 / jax.random.uniform(quick_random_key, (KV_HEADS,), jnp.float32, 30.0, 100.0)
    rate = jnp.where(gradual_decay, slow_rate, fast_rate)
    factor = jnp.exp(jax.random.uniform(block_random_key, (FIRST_TOKENS // SEQ_ROWS,), jnp.float32, -0.7, 0.7))
    per_position = jnp.repeat(factor, SEQ_ROWS)
    update_steps = -rate[:, None] * per_position[None, :] * rough
    marked_positions = jax.random.randint(spike_random_key, (2,), 0, FIRST_TOKENS)
    loss_values = jnp.log(jax.random.uniform(loss_random_key, (2,), jnp.float32, 0.5, 0.8))
    sudden_spike = jnp.zeros((FIRST_TOKENS,), jnp.float32).at[marked_positions].add(loss_values)
    update_steps = update_steps + jnp.where(gradual_decay[:, None], sudden_spike[None, :], 0.0)
    return jnp.cumsum(update_steps, axis=1)


def block_scale(stream_key, shape, cuts, low, largest):
    gain, own = 1.0, jax.random.fold_in(stream_key, 6)
    for dim, shards_of in cuts:
        draws = jnp.exp(jax.random.uniform(jax.random.fold_in(own, dim), (shards_of,), jnp.float32, low / len(cuts), largest / len(cuts)))
        gain = gain * jnp.repeat(draws, shape[dim] // shards_of).reshape([-1 if axis == dim else 1 for axis in range(len(shape))])
    return gain


def routed_block(stream_key, own, number, rows, count, top, bound, lean):
    order = jax.random.permutation(stream_key, count)
    packed, usual = load_shares(count, rows * top, bound, lean, True), load_shares(count, rows * top, bound, lean, False)
    places = jnp.arange(count)

    def named(sizes, turn):
        used = int((sizes > 0).sum())
        fixed = max(1, used // 4)
        passed = fixed + (places - fixed + turn * (used - fixed)) % max(1, count - fixed)
        return jnp.zeros((count,), jnp.int32).at[order[jnp.where(places < fixed, places, passed)]].set(jnp.asarray(sizes, jnp.int32))

    sizes = jnp.where(number % 4 == 0, named(packed, number // 4), named(usual, number - number // 4 - 1))
    mixed = jax.random.permutation(jax.random.fold_in(own, 3), count)
    donor, taker = mixed[0:count // 2 * 2:2], mixed[1:count // 2 * 2:2]
    margin = jnp.minimum(sizes[donor] - 1, bound - sizes[taker]) // 2
    margin = jnp.where((donor == order[0]) | (taker == order[0]) | (sizes[taker] == 0), 0, jnp.maximum(margin, 0))
    passed = jax.random.randint(jax.random.fold_in(own, 4), (count // 2,), 0, 1 << 20) % (margin + 1)
    sizes = sizes.at[donor].add(-passed).at[taker].add(passed)
    members = jnp.searchsorted(jnp.cumsum(sizes), jnp.arange(rows * top), side="right").astype(jnp.int32)
    table = members.reshape(top, rows).T
    table = table[jax.random.permutation(jax.random.fold_in(own, 1), rows)]
    turn = jax.random.randint(jax.random.fold_in(own, 2), (rows, 1), 0, top)
    return jnp.take_along_axis(table, (jnp.arange(top)[None, :] + turn) % top, axis=1)


def load_shares(amount, total, bound, slope, full):
    loads = [(1 << 20) // math.isqrt(rank ** slope) + 1 for rank in range(1, amount + 1)]
    largest = bound if full else min(bound, max(-(-total // amount), total * loads[0] // sum(loads)))
    least = 1 if total - largest >= amount - 1 else 0
    counts, spare = [largest] + [least] * (amount - 1), total - largest - least * (amount - 1)
    while spare > 0:
        movable = [i for i in range(1, amount) if counts[i] < largest] or [i for i in range(1, amount) if counts[i] < bound]
        whole, budget = sum([loads[i] for i in movable]), spare
        for i in movable:
            addition = min(bound - counts[i], max(1, budget * loads[i] // whole), spare)
            counts[i] = counts[i] + addition
            spare = spare - addition
    return np.array(counts)


def centred(key, dims, spread, bound, pieces=(), kind=jnp.bfloat16):
    result = jax.random.normal(key, dims, jnp.float32) * spread
    if len(pieces) > 0:
        result = block_scale(key, dims, pieces, -0.22, 0.18) * result
    return jnp.clip(result, min=-bound, max=bound).astype(kind)


def setup_inputs(seed: int = 0) -> dict:
    keys = jax.random.split(jax.random.key(seed), 13)
    queries = draw_queries(jax.random.fold_in(keys[12], 71), 0)
    key_cache = draw_key_cache(jax.random.fold_in(keys[12], 71), 0)
    value_cache = centred(keys[2], (KV_HEADS, HEAD, FIRST_TOKENS), 1.0, 6.0, ((0, 4), (2, 8)))
    cum_gate = draw_cum_gate(jax.random.fold_in(keys[12], 71), 0)
    out_weight = centred(keys[4], (HEADS * HEAD, D), (HEADS * HEAD // 16) ** -0.5, 1.0)
    routed_input = centred(keys[5], (ROUTED_TOKENS, D), 1.0, 6.0, ((0, 8),))
    norm_gain = jnp.clip(1.0 + 0.18 * jax.random.normal(keys[6], (D,), jnp.float32), 0.099609375, 1.8984375).astype(jnp.bfloat16)
    routes_keys = jax.random.split(jax.random.fold_in(keys[7], 1), ROUTED_TOKENS // TOK_DEV)
    routes_turns = jax.random.permutation(jax.random.fold_in(keys[7], 3), ROUTED_TOKENS // TOK_DEV)
    routes = jax.vmap(lambda own, number: routed_block(jax.random.fold_in(keys[7], 2), own, number, TOK_DEV, EXPERTS, TOPK, CAP, 1))(routes_keys, routes_turns).reshape((ROUTED_TOKENS, TOPK))
    route_weight = jnp.clip(0.2 + 0.8 * jax.random.uniform(keys[8], (ROUTED_TOKENS, TOPK), jnp.float32) ** block_scale(keys[8], (ROUTED_TOKENS, TOPK), ((0, 8),), -0.2, 0.2), 0.2, 1.0)
    expert_gate = centred(keys[9], (EXPERTS, D, FFE), D ** -0.5, 0.125, ((0, 8), (2, 4)))
    expert_up = centred(keys[10], (EXPERTS, D, FFE), D ** -0.5, 0.125, ((0, 8), (2, 4)))
    expert_down = centred(keys[11], (EXPERTS, FFE, D), FFE ** -0.5, 0.1875, ((0, 8), (1, 4)))
    return dict(queries=queries, key_cache=key_cache, value_cache=value_cache, cum_gate=cum_gate, out_weight=out_weight, routed_input=routed_input, norm_gain=norm_gain, routes=routes, route_weight=route_weight, expert_gate=expert_gate, expert_up=expert_up, expert_down=expert_down)


def attend_block(query_block, keys_head, values_head, gate_head, block_start):
    rows_here = query_block.shape[0]
    scores = jnp.einsum('tgd,ds->tgs', query_block, keys_head) * HEAD ** (-0.5)
    query_pos = block_start + jnp.arange(rows_here, dtype=jnp.int32)
    gate_query = lax.dynamic_slice_in_dim(gate_head, block_start, rows_here, 0)
    scores = scores + gate_query[:, None, None] - gate_head[None, None, :]
    key_pos = jnp.arange(FIRST_TOKENS, dtype=jnp.int32)
    allowed = key_pos[None, :] <= query_pos[:, None]
    scores = jnp.where(allowed[:, None, :], scores, -jnp.inf)
    highest = lax.optimization_barrier(jnp.max(scores, axis=-1, keepdims=True))
    weights = jnp.exp(scores - highest)
    total = lax.optimization_barrier(jnp.sum(weights, axis=-1))
    rounded = lax.optimization_barrier(weights.astype(jnp.bfloat16)).astype(jnp.float32)
    summed = jnp.einsum('tgs,ds->tgd', rounded, values_head)
    return (summed / total[..., None]).astype(jnp.bfloat16)

def reference(queries, key_cache, value_cache, cum_gate, out_weight, routed_input, norm_gain, routes, route_weight, expert_gate, expert_up, expert_down):
    group = HEADS // KV_HEADS
    nblocks = FIRST_TOKENS // SEQ_ROWS
    query_all = queries.astype(jnp.float32).reshape(nblocks, SEQ_ROWS, KV_HEADS, group, HEAD)
    keys_all = key_cache.astype(jnp.float32)
    values_all = value_cache.astype(jnp.float32)

    def one_pair(index):
        block = index // KV_HEADS
        head = index % KV_HEADS
        query_block = query_all[block, :, head]
        start = (block * SEQ_ROWS).astype(jnp.int32)
        return attend_block(query_block, keys_all[head], values_all[head], cum_gate[head], start)
    attended = lax.map(one_pair, jnp.arange(nblocks * KV_HEADS, dtype=jnp.int32))
    attended = attended.reshape(nblocks, KV_HEADS, SEQ_ROWS, group, HEAD).transpose(0, 2, 1, 3, 4).reshape(FIRST_TOKENS, HEADS * HEAD)
    mixed_out = jnp.dot(attended, out_weight, preferred_element_type=jnp.float32).astype(jnp.bfloat16)
    source = routed_input.astype(jnp.float32)
    scale = lax.rsqrt(lax.optimization_barrier(jnp.mean(source * source, axis=-1, keepdims=True)) + 1e-06)
    normed = (source * scale * norm_gain.astype(jnp.float32)).astype(jnp.bfloat16)
    nparts = ROUTED_TOKENS // TOK_DEV
    slots_all = EXPERTS * CAP
    pairs = routes.reshape(nparts, TOK_DEV * TOPK)
    same = (pairs[:, :, None] == jnp.arange(EXPERTS, dtype=jnp.int32)[None, None, :]).astype(jnp.int32)
    earlier = jnp.cumsum(same, axis=1) - same
    rank = lax.optimization_barrier(jnp.sum(earlier * same, axis=2))
    slot = pairs * CAP + rank
    chooser = (slot[:, :, None] == jnp.arange(slots_all, dtype=jnp.int32)[None, None, :]).astype(jnp.float32)
    chooser = chooser.reshape(nparts, TOK_DEV, TOPK, slots_all)
    normed_blocks = normed.astype(jnp.float32).reshape(nparts, TOK_DEV, D)
    width_part = FFE // N_TP

    def one_expert(expert):
        picks = lax.dynamic_slice_in_dim(chooser, expert * CAP, CAP, 3)
        gathered = jnp.einsum('btkc,btd->bcd', picks, normed_blocks).astype(jnp.bfloat16).reshape(nparts * CAP, D)
        gate = jnp.dot(gathered, expert_gate[expert], preferred_element_type=jnp.float32)
        upper = jnp.dot(gathered, expert_up[expert], preferred_element_type=jnp.float32)
        hidden = (jax.nn.silu(gate) * upper).astype(jnp.bfloat16)
        hidden_parts = hidden.astype(jnp.float32).reshape(nparts * CAP, N_TP, width_part)
        down_parts = expert_down[expert].astype(jnp.float32).reshape(N_TP, width_part, D)
        partial_value = jnp.einsum('rqf,qfd->qrd', hidden_parts, down_parts)
        partial_value = lax.optimization_barrier(partial_value.astype(jnp.bfloat16)).astype(jnp.float32)
        return lax.optimization_barrier(jnp.sum(partial_value, axis=0)).astype(jnp.bfloat16).reshape(nparts, CAP, D)
    results = lax.map(one_expert, jnp.arange(EXPERTS, dtype=jnp.int32))
    rank_blocks = rank.reshape(nparts, TOK_DEV, TOPK)
    expert_blocks = routes.reshape(nparts, TOK_DEV, TOPK)
    block_ids = jnp.arange(nparts, dtype=jnp.int32)[:, None, None]
    picked = results[expert_blocks, block_ids, rank_blocks].astype(jnp.float32)
    mixed_weights = route_weight.reshape(nparts, TOK_DEV, TOPK)[..., None] * picked
    expert_out = lax.optimization_barrier(jnp.sum(mixed_weights, axis=2)).reshape(ROUTED_TOKENS, D).astype(jnp.bfloat16)
    return (mixed_out, expert_out)
```

```python
import functools

import jax
import jax.numpy as jnp
from jax import lax
from jax.experimental import pallas as pl
from jax.experimental.pallas import tpu as pltpu
from jax.sharding import PartitionSpec as P

MESH = pl.DeviceIdType.MESH


INNER_SENDS = (1, 3, 2)
OUTER_SENDS = (3, 1, 2)
LAND_SENDS = (3, 1, 2)
INNER_STEPS = (
    "C0", "D0", "E0", "A1", "L1", "A6", "C1", "D1", "L0", "A7", "B6", "K", "C6", "A4",
    "A2", "A3", "E1", "D6", "B7", "C7", "B4", "D7", "A5", "C3", "E6", "C4", "T", "E7",
    "D4", "D3", "C2", "B5", "C5", "D2", "E4", "E3", "D5", "E2", "E5",
)
OUTER_STEPS = (
    "C0", "D0", "A3", "E0", "C3", "A1", "A2", "D3", "C1", "A7", "C2", "A6", "E3", "B7",
    "A5", "A4", "C7", "B6", "D7", "C6", "B5", "K", "D6", "D2", "E7", "C5", "B4", "C4",
    "D5", "D1", "E6", "D4", "E5", "E2", "T", "E1", "E4",
)


def fused_kernel(
    n,
    tpn,
    cap,
    q_any,
    gate_any,
    gain_any,
    routes_any,
    rw_any,
    k_any,
    v_any,
    ow_any,
    x_any,
    wg_any,
    wu_any,
    wd_any,
    mixed_ref,
    out_ref,
    q_ref,
    gate_ref,
    gain_ref,
    routes_ref,
    rw_ref,
    xbuf,
    wgv,
    wuv,
    wdv,
    owv,
    kv,
    att,
    attr,
    sel,
    raw,
    land,
    lroutes,
    sbuf,
    sland,
    recv,
    part,
    r1,
    s2,
    r2,
    s3,
    rbuf,
    lsem,
    kvs,
    kvr,
    ats,
    atr,
    w_s,
    w_r,
    a_s,
    a_r,
    l_s,
    bx_s,
    bx_r,
    f_s,
    f_r,
    r1_s,
    r1_r,
    r2_s,
    r2_r,
    r3_s,
    r3_r,
):
    e = lax.axis_index("ep")
    t = lax.axis_index("tp")
    partner = t + 1 - 2 * lax.rem(t, 2)
    peer = lax.rem(t + 2, tpn)
    opp = lax.rem(partner + 2, tpn)
    mate = e + 1 - 2 * lax.rem(e, 2)
    half = n // 2
    _, own_rows, width = xbuf.shape
    wide = width // 2
    head = k_any.shape[1]
    seq = q_ref.shape[0]

    side = lax.div(e, half)
    base = side * half
    local = lax.rem(e, half)
    row = lax.rem(e, 2)
    inner = lax.div(local, 2) == 1 - side
    rank = jnp.where(inner, 0, 1)

    barrier = pltpu.get_barrier_semaphore()
    for s in range(1, n):
        pl.semaphore_signal(
            barrier, inc=1, device_id={"ep": lax.rem(e + s, n), "tp": t}, device_id_type=MESH
        )
    for s in range(1, tpn):
        pl.semaphore_signal(
            barrier, inc=1, device_id={"ep": e, "tp": lax.rem(t + s, tpn)}, device_id_type=MESH
        )

    blocks = (t, peer, partner, opp)

    def load_x(j):
        at = blocks[j] * own_rows
        return pltpu.make_async_copy(x_any.at[pl.ds(at, own_rows)], xbuf.at[j], lsem.at[12 + j])

    load_k = pltpu.make_async_copy(k_any.at[0], kv.at[e, pl.ds(0, head)], lsem.at[1])
    load_v = pltpu.make_async_copy(v_any.at[0], kv.at[e, pl.ds(head, head)], lsem.at[2])
    load_g = pltpu.make_async_copy(wg_any.at[0], wgv, lsem.at[3])
    load_u = pltpu.make_async_copy(wu_any.at[0], wuv, lsem.at[4])
    load_d = pltpu.make_async_copy(wd_any.at[0], wdv, lsem.at[5])
    load_o = pltpu.make_async_copy(ow_any, owv, lsem.at[6])
    load_q = pltpu.make_async_copy(q_any, q_ref, lsem.at[8])
    load_c = pltpu.make_async_copy(gate_any, gate_ref, lsem.at[9])
    load_n = pltpu.make_async_copy(gain_any, gain_ref, lsem.at[10])
    load_r = pltpu.make_async_copy(routes_any, routes_ref, lsem.at[11])
    load_w = pltpu.make_async_copy(rw_any, rw_ref, lsem.at[0])
    load_r.start()
    load_n.start()
    load_x(0).start()
    load_x(1).start()
    load_k.start()
    load_v.start()
    for j in range(2, tpn):
        load_x(j).start()
    load_g.start()
    load_u.start()
    load_d.start()
    load_w.start()
    load_q.start()
    load_c.start()
    load_o.start()

    def remote(src, dst, ssem, rsem, ep, tp):
        return pltpu.make_async_remote_copy(
            src_ref=src,
            dst_ref=dst,
            send_sem=ssem,
            recv_sem=rsem,
            device_id={"ep": ep, "tp": tp},
            device_id_type=MESH,
        )

    def flip(s):
        s = jnp.int32(s)
        flipped = jnp.int32(0)
        bit = 1
        while bit < n:
            ours = lax.rem(lax.div(e, jnp.int32(bit)), jnp.int32(2))
            theirs = lax.rem(lax.div(s, jnp.int32(bit)), jnp.int32(2))
            flipped = flipped + bit * (ours + theirs - 2 * ours * theirs)
            bit *= 2
        return flipped

    def kv_far(s):
        return remote(kv.at[e], kv.at[e], kvs.at[s], kvr.at[s], lax.rem(e + 2 * s, n), t)

    def kv_far_in(s):
        src = lax.rem(e - 2 * s + n, n)
        return remote(kv.at[src], kv.at[src], kvs.at[s], kvr.at[s], lax.rem(e + 2 * s, n), t)

    def kv_mate(s):
        src = lax.rem(e - 2 * s + n, n)
        return remote(kv.at[src], kv.at[src], kvs.at[half + s], kvr.at[half + s], mate, t)

    def kv_mate_in(s):
        src = lax.rem(mate - 2 * s + n, n)
        return remote(kv.at[src], kv.at[src], kvs.at[half + s], kvr.at[half + s], mate, t)

    def far_sends(s):
        return e + 2 * s < n

    def far_comes(s):
        return e - 2 * s >= 0

    def mate_sends(s):
        return (e - 2 * s >= 0) if s else row == 0

    def mate_comes(s):
        return (mate - 2 * s >= 0) if s else row == 1

    across = (2 - side) * 2 + row
    send_raw = remote(raw, land.at[rank], w_s.at[0], w_r.at[rank], across, t)
    send_routes = remote(routes_ref, lroutes.at[rank], w_s.at[1], w_r.at[2 + rank], across, t)

    def raw_in(j):
        return remote(raw, land.at[j], w_s.at[0], w_r.at[j], across, t)

    def routes_in(j):
        return remote(routes_ref, lroutes.at[j], w_s.at[1], w_r.at[2 + j], across, t)

    def near(s):
        dst = flip(s)
        return remote(
            sbuf.at[lax.rem(dst, half)],
            recv.at[s, pl.ds(0, 2)],
            a_s.at[s],
            a_r.at[s],
            dst,
            t,
        )

    def landed(j, s):
        dst = flip(s)
        return remote(
            sland.at[j, lax.rem(dst, half)],
            recv.at[half + 2 * j + s % 2, 0],
            l_s.at[j, s],
            a_r.at[half + 2 * j + s % 2],
            dst,
            t,
        )

    def landed_in(g):
        return remote(sland.at[0, 0], recv.at[g, 0], l_s.at[0, 0], a_r.at[g], e, peer)

    def copy_bx(g):
        return remote(recv.at[g, 0], recv.at[g, 1], bx_s.at[g], bx_r.at[g], e, peer)

    def copy_f(g):
        return remote(
            recv.at[g, pl.ds(0, 2)], recv.at[g, pl.ds(2, 2)], f_s.at[g], f_r.at[g], e, partner
        )

    def copy_r1(g):
        return remote(part.at[g, pl.ds(2, 2)], r1.at[g], r1_s.at[g], r1_r.at[g], e, partner)

    def copy_r2(g):
        return remote(s2.at[g], r2.at[g], r2_s.at[g], r2_r.at[g], e, peer)

    def source(g):
        g = jnp.int32(g)
        which = lax.div(g - half, jnp.int32(2))
        turn = lax.rem(g, jnp.int32(2))
        z = jnp.where(side == 0, 2 + which, 1 - which)
        far = 2 * z + row + turn - 2 * row * turn
        return jnp.where(g < half, flip(g), far)

    def copy_r3(g):
        return remote(s3.at[g], rbuf.at[e], r3_s.at[g], r3_r.at[e], source(g), t)

    def copy_r3_in(s):
        src = flip(s)
        return remote(s3.at[0], rbuf.at[src], r3_s.at[0], r3_r.at[src], src, t)

    top, share = routes_ref.shape

    def column(line, block):
        at = block * own_rows
        own = lax.broadcasted_iota(jnp.int32, (own_rows, share), 1) == (
            lax.broadcasted_iota(jnp.int32, (own_rows, share), 0) + at
        )
        return jnp.sum(
            jnp.where(own, jnp.broadcast_to(line, own.shape), 0.0), axis=1, keepdims=True
        )

    def named_by(ref, block):
        return [column(ref[k : k + 1, :].astype(jnp.float32), block) for k in range(top)]

    before = lax.broadcasted_iota(jnp.int32, (own_rows, own_rows), 1) < lax.broadcasted_iota(
        jnp.int32, (own_rows, own_rows), 0
    )

    def lanes_of(first, count):
        lanes = 2 * count * cap
        place = lax.broadcasted_iota(jnp.int32, (own_rows, lanes), 1).astype(jnp.float32) + 0.5
        expert = jnp.floor(place / (2.0 * cap))
        inside = place - 0.5 - expert * (2.0 * cap)
        right = inside >= cap
        slot = jnp.where(right, inside - cap, inside)
        return expert + first.astype(jnp.float32), right, slot

    def hits_of(names, lanes):
        expert, right, slot = lanes
        named = [name == expert for name in names]
        total = sum([m.astype(jnp.float32) for m in named])
        ranks = jnp.dot(
            before.astype(jnp.bfloat16),
            total.astype(jnp.bfloat16),
            preferred_element_type=jnp.float32,
        )
        return named, total, ranks == slot

    def spread_of(names, lanes):
        _, total, hit = hits_of(names, lanes)
        right = lanes[1]
        chosen = jnp.where(hit, total, 0.0)
        spread = jnp.concatenate(
            [jnp.where(right, 0.0, chosen), jnp.where(right, chosen, 0.0)], axis=0
        )
        return spread.T.astype(jnp.bfloat16)

    def chunks(spread, rows):
        return jnp.dot(spread, rows, preferred_element_type=jnp.float32).astype(jnp.bfloat16)

    load_r.wait()
    side_lanes = lanes_of(base, half)
    own_names = named_by(routes_ref, t)
    spread = spread_of(own_names, side_lanes)
    load_n.wait()
    gain = gain_ref[...].astype(jnp.float32)
    gain = jnp.concatenate([gain[j : j + 1, :] for j in range(gain.shape[0])], axis=1)

    def halves(j):
        load_x(j).wait()
        x = xbuf[j].astype(jnp.float32)
        scale = lax.rsqrt(jnp.mean(x * x, axis=-1, keepdims=True) + 1e-06)
        normed = (x * scale * gain).astype(jnp.bfloat16)
        return jnp.concatenate([normed[:, :wide], normed[:, wide:]], axis=0)

    own = halves(0)
    raw[...] = own
    sbuf[:, 0] = chunks(spread, own).reshape(half, 2 * cap, wide)

    with jax.named_scope("barrier"):
        pl.semaphore_wait(barrier, n - 1 + tpn - 1)
    send_raw.start()
    send_routes.start()
    sbuf[:, 1] = chunks(spread_of(named_by(routes_ref, peer), side_lanes), halves(1)).reshape(
        half, 2 * cap, wide
    )
    @pl.when(inner)
    def _():
        for s in INNER_SENDS:
            near(s).start()

    @pl.when(jnp.logical_not(inner))
    def _():
        for s in OUTER_SENDS:
            near(s).start()

    load_k.wait()
    load_v.wait()
    for s in range(1, half):

        @pl.when(far_sends(s))
        def _():
            kv_far(s).start()

    @pl.when(mate_sends(0))
    def _():
        kv_mate(0).start()

    own_lanes = lanes_of(e, 1)
    recv[0, 0:2] = sbuf[local]
    for j in (2, 3):
        recv[0, j] = chunks(spread_of(named_by(routes_ref, blocks[j]), own_lanes), halves(j))

    def copy_att(s):
        dst = lax.rem(t + s, tpn)
        return remote(att.at[dst], attr.at[t], ats.at[s], atr.at[s], e, dst)

    def copy_att_in(s):
        src = lax.rem(t - s + tpn, tpn)
        return remote(att.at[src], attr.at[src], ats.at[s], atr.at[s], e, lax.rem(t + s, tpn))

    def attention():
        for s in range(half):

            @pl.when(mate_comes(s))
            def _():
                kv_mate_in(s).wait_recv()

        for j in range(1, n):

            @pl.when(j > e)
            def _():
                kv[j] = jnp.zeros(kv.shape[1:], kv.dtype)

        load_q.wait()
        load_c.wait()
        own_gate = gate_ref[:, pl.ds(pl.multiple_of(e * seq, seq), seq)]
        eye = lax.broadcasted_iota(jnp.int32, (seq, seq), 0) == lax.broadcasted_iota(
            jnp.int32, (seq, seq), 1
        )
        gate_col = jnp.sum(
            jnp.where(eye, jnp.broadcast_to(own_gate, (seq, seq)), 0.0), axis=1, keepdims=True
        )
        key_pos = lax.broadcasted_iota(jnp.int32, (seq, n * seq), 1)
        query_pos = lax.broadcasted_iota(jnp.int32, (seq, n * seq), 0) + e * seq
        bias = gate_col - gate_ref[...]
        group = q_ref.shape[1] // head
        heads_out = []
        for g in range(group):
            q = q_ref[:, g * head : (g + 1) * head]
            scores = jnp.concatenate(
                [
                    jnp.dot(q, kv[j, 0:head, :], preferred_element_type=jnp.float32)
                    for j in range(n)
                ],
                axis=1,
            )
            scores = scores * (head ** (-0.5)) + bias
            scores = jnp.where(key_pos <= query_pos, scores, -jnp.inf)
            weights = jnp.exp(scores - jnp.max(scores, axis=-1, keepdims=True))
            whole = jnp.sum(weights, axis=-1, keepdims=True)
            weights = weights.astype(jnp.bfloat16)
            summed = jnp.zeros((seq, head), jnp.float32)
            for j in range(n):
                summed = summed + lax.dot_general(
                    weights[:, j * seq : (j + 1) * seq],
                    kv[j, head : 2 * head, :],
                    (((1,), (1,)), ((), ())),
                    preferred_element_type=jnp.float32,
                )
            heads_out.append(summed / whole)
        attended = jnp.concatenate(heads_out, axis=1).astype(jnp.bfloat16)
        att[...] = attended.reshape(att.shape)
        attr[t] = att[t]
        for s in range(1, tpn):
            copy_att(s).start()

    def pass_kv():
        for s in range(1, half):

            @pl.when(far_comes(s))
            def _():
                kv_far_in(s).wait_recv()
                kv_mate(s).start()

    def land_rows(j):
        with jax.named_scope(f"w_land{j}"):
            raw_in(j).wait_recv()
            routes_in(j).wait_recv()
        names = named_by(lroutes.at[j], t)
        sland[j] = chunks(spread_of(names, side_lanes), land[j]).reshape(half, 2 * cap, wide)
        for s in LAND_SENDS:
            landed(j, s).start()
        recv[half + 2 * j, 0] = sland[j, local]

    def arrive(g, here):
        if g < half:
            near_in(g).wait_recv()
            copy_f(g).start()
        else:
            if not here or g % 2:
                landed_in(g).wait_recv()
            copy_bx(g).start()

    def near_in(g):
        return remote(
            sbuf.at[0], recv.at[g, pl.ds(0, 2)], a_s.at[0], a_r.at[g], e, peer
        )

    def spread_pair(g):
        copy_bx(g).wait_recv()
        copy_f(g).start()

    def experts(g):
        if g:
            with jax.named_scope(f"w_f{g}"):
                copy_f(g).wait_recv()
        block = recv[g].astype(jnp.float32)
        count = block.shape[0] * cap
        lo = block[:, :cap].reshape(count, wide).astype(jnp.bfloat16)
        hi = block[:, cap:].reshape(count, wide).astype(jnp.bfloat16)
        gate = jnp.dot(lo, wgv[0:wide, :], preferred_element_type=jnp.float32) + jnp.dot(
            hi, wgv[wide:, :], preferred_element_type=jnp.float32
        )
        upper = jnp.dot(lo, wuv[0:wide, :], preferred_element_type=jnp.float32) + jnp.dot(
            hi, wuv[wide:, :], preferred_element_type=jnp.float32
        )
        hidden = (gate / (1.0 + jnp.exp(-gate)) * upper).astype(jnp.bfloat16)
        down = jnp.dot(hidden, wdv[...], preferred_element_type=jnp.float32)
        shape = (tpn, cap, wide)
        part[g] = jnp.concatenate(
            [down[:, :wide].reshape(shape), down[:, wide:].reshape(shape)], axis=1
        ).astype(jnp.bfloat16)
        copy_r1(g).start()

    def cross(g):
        copy_r1(g).wait_recv()
        s2[g] = (part[g, 1].astype(jnp.float32) + r1[g, 1].astype(jnp.float32)).astype(
            jnp.bfloat16
        )
        copy_r2(g).start()

    def give_back(g):
        copy_r2(g).wait_recv()
        done = (
            part[g, 0].astype(jnp.float32)
            + r1[g, 0].astype(jnp.float32)
            + r2[g].astype(jnp.float32)
        ).astype(jnp.bfloat16)
        if g == 0:
            rbuf[e] = done
        else:
            s3[g] = done
            copy_r3(g).start()

    def first_matmul():
        load_g.wait()
        load_u.wait()
        load_d.wait()

    def choose_back():
        everywhere = lanes_of(e * 0, n)
        named, _, hit = hits_of(own_names, everywhere)
        right = everywhere[1]
        for k in range(top):
            mine = jnp.where(hit & named[k], 1.0, 0.0)
            sel[2 * k * own_rows : (2 * k + 1) * own_rows, :] = jnp.where(
                right, 0.0, mine
            ).astype(jnp.bfloat16)
            sel[(2 * k + 1) * own_rows : (2 * k + 2) * own_rows, :] = jnp.where(
                right, mine, 0.0
            ).astype(jnp.bfloat16)

    def run(steps, here):
        for name in steps:
            kind = name[0]
            with jax.named_scope(name):
                if kind == "L":
                    land_rows(int(name[1:]))
                elif kind == "K":
                    pass_kv()
                elif kind == "T":
                    attention()
                elif kind == "A":
                    arrive(int(name[1:]), here)
                else:
                    {"B": spread_pair, "C": experts, "D": cross, "E": give_back}[kind](
                        int(name[1:])
                    )

    first_matmul()

    @pl.when(inner)
    def _():
        run(INNER_STEPS, True)

    @pl.when(jnp.logical_not(inner))
    def _():
        run(OUTER_STEPS, False)

    choose_back()

    with jax.named_scope("w_att"):
        for s in range(1, tpn):
            copy_att_in(s).wait_recv()
        load_o.wait()
    joined = jnp.concatenate([attr[j] for j in range(tpn)], axis=1)
    mixed_ref[...] = jnp.dot(joined, owv[...], preferred_element_type=jnp.float32).astype(
        jnp.bfloat16
    )
    load_w.wait()
    rw = [column(rw_ref[k : k + 1, :], t) for k in range(top)]

    send_raw.wait_send()
    send_routes.wait_send()
    for s in range(1, half):
        near(s).wait_send()

        @pl.when(far_sends(s))
        def _():
            kv_far(s).wait_send()

        @pl.when(inner)
        def _():
            for j in range(2):
                landed(j, s).wait_send()

    for s in range(half):

        @pl.when(mate_sends(s))
        def _():
            kv_mate(s).wait_send()

    for s in range(1, tpn):
        copy_att(s).wait_send()

    def drain(g, carry):
        @pl.when(g > 0)
        def _():
            copy_f(g).wait_send()

        @pl.when(g >= half)
        def _():
            copy_bx(g).wait_send()

        copy_r1(g).wait_send()
        copy_r2(g).wait_send()
        return carry

    lax.fori_loop(0, n, drain, 0)

    with jax.named_scope("w_r3"):
        for s in range(1, n):
            copy_r3_in(s).wait_recv()
    lanes = 2 * n * cap
    picked = jnp.dot(
        sel[...], rbuf[...].reshape(lanes, wide), preferred_element_type=jnp.float32
    )
    for h in range(2):
        acc = jnp.zeros((own_rows, wide), jnp.float32)
        for k in range(top):
            at = (2 * k + h) * own_rows
            acc = acc + rw[k] * picked[at : at + own_rows]
        out_ref[:, h * wide : (h + 1) * wide] = acc.astype(jnp.bfloat16)

    def last(g, carry):
        copy_r3(g).wait_send()
        return carry

    lax.fori_loop(1, n, last, 0)


def fused_body(
    n,
    tpn,
    queries,
    key_cache,
    value_cache,
    cum_gate,
    out_weight,
    routed_input,
    norm_gain,
    routes,
    route_weight,
    expert_gate,
    expert_up,
    expert_down,
):
    seq = queries.shape[0]
    head = key_cache.shape[1]
    width = routed_input.shape[1]
    wide = width // 2
    own_rows = routed_input.shape[0] // tpn
    top = routes.shape[1]
    units = expert_gate.shape[2]
    cap = block_capacity(own_rows, top, n * expert_gate.shape[0])
    half = n // 2
    bf16 = jnp.bfloat16
    chunk = (2 * cap, wide)
    anywhere = pl.BlockSpec(memory_space=pltpu.HBM)
    vmem = pl.BlockSpec(memory_space=pltpu.VMEM)
    dma = pltpu.SemaphoreType.DMA
    mixed, out = pl.pallas_call(
        functools.partial(fused_kernel, n, tpn, cap),
        out_shape=(
            pltpu.VMEM((seq // tpn, width), bf16),
            pltpu.VMEM((own_rows, width), bf16),
        ),
        in_specs=[anywhere] * 12,
        out_specs=(vmem, vmem),
        scratch_shapes=[
            pltpu.VMEM(queries.shape, bf16),
            pltpu.VMEM(cum_gate.shape, jnp.float32),
            pltpu.VMEM((width // 128, 128), bf16),
            pltpu.VMEM((top, tpn * own_rows), jnp.int32),
            pltpu.VMEM((top, tpn * own_rows), jnp.float32),
            pltpu.VMEM((tpn, own_rows, width), bf16),
            pltpu.VMEM((width, units), bf16),
            pltpu.VMEM((width, units), bf16),
            pltpu.VMEM((units, width), bf16),
            pltpu.VMEM(out_weight.shape, bf16),
            pltpu.VMEM((n, 2 * head, seq), bf16),
            pltpu.VMEM((tpn, seq // tpn, queries.shape[1]), bf16),
            pltpu.VMEM((tpn, seq // tpn, queries.shape[1]), bf16),
            pltpu.VMEM((2 * top * own_rows, 2 * n * cap), bf16),
            pltpu.VMEM((2 * own_rows, wide), bf16),
            pltpu.VMEM((2, 2 * own_rows, wide), bf16),
            pltpu.VMEM((2, top, tpn * own_rows), jnp.int32),
            pltpu.VMEM((half, 2) + chunk, bf16),
            pltpu.VMEM((2, half) + chunk, bf16),
            pltpu.VMEM((n, tpn) + chunk, bf16),
            pltpu.VMEM((n, tpn) + chunk, bf16),
            pltpu.VMEM((n, 2) + chunk, bf16),
            pltpu.VMEM((n,) + chunk, bf16),
            pltpu.VMEM((n,) + chunk, bf16),
            pltpu.VMEM((n,) + chunk, bf16),
            pltpu.VMEM((n,) + chunk, bf16),
            dma((12 + tpn,)),
            dma((n,)),
            dma((n,)),
            dma((tpn,)),
            dma((tpn,)),
            dma((2,)),
            dma((4,)),
            dma((half,)),
            dma((n,)),
            dma((2, half)),
        ]
        + [dma((n,))] * 10,
        compiler_params=pltpu.CompilerParams(
            collective_id=0, has_side_effects=True, vmem_limit_bytes=60 * 1024 * 1024
        ),
    )(
        queries,
        cum_gate,
        norm_gain.reshape(width // 128, 128),
        routes.T,
        route_weight.T,
        key_cache,
        value_cache,
        out_weight,
        routed_input,
        expert_gate,
        expert_up,
        expert_down,
    )
    return write_out(mixed, out)


def write_kernel(a, b, a_out, b_out, sem):
    copies = [
        pltpu.make_async_copy(a, a_out, sem.at[0]),
        pltpu.make_async_copy(b, b_out, sem.at[1]),
    ]
    for copy in copies:
        copy.start()
    for copy in copies:
        copy.wait()


def write_out(*arrays):
    return pl.pallas_call(
        write_kernel,
        out_shape=[jax.ShapeDtypeStruct(a.shape, a.dtype) for a in arrays],
        in_specs=[pl.BlockSpec(memory_space=pltpu.VMEM)] * len(arrays),
        out_specs=[pl.BlockSpec(memory_space=pltpu.HBM)] * len(arrays),
        scratch_shapes=[pltpu.SemaphoreType.DMA((len(arrays),))],
    )(*[pltpu.with_memory_space_constraint(a, pltpu.VMEM) for a in arrays])


def block_capacity(own_rows, top_count, expert_count):
    return max(2, own_rows * top_count * 3 // (2 * expert_count))


def slot_chooser(route_rows, expert_count, capacity):
    token_rows, top_count = route_rows.shape
    flat = route_rows.reshape(token_rows * top_count)
    same = (flat[:, None] == jnp.arange(expert_count, dtype=jnp.int32)[None, :]).astype(jnp.int32)
    earlier = jnp.cumsum(same, axis=0) - same
    rank = jnp.sum(earlier * same, axis=1)
    slot = flat * capacity + rank
    chosen = slot[:, None] == jnp.arange(expert_count * capacity, dtype=jnp.int32)[None, :]
    return chosen.astype(jnp.bfloat16).reshape(token_rows, top_count, expert_count * capacity)


def rms_rows(source, norm_gain):
    widened = source.astype(jnp.float32)
    scale = lax.rsqrt(jnp.mean(widened * widened, axis=-1, keepdims=True) + 1e-06)
    return (widened * scale * norm_gain.astype(jnp.float32)).astype(jnp.bfloat16)


def mixer_half(queries, key_cache, value_cache, cum_gate, out_weight):
    seq_rows = queries.shape[0]
    local_heads = key_cache.shape[0]
    head_size = key_cache.shape[1]
    group = queries.shape[1] // (local_heads * head_size)
    own_start = lax.axis_index("ep") * seq_rows
    query_heads = queries.reshape(seq_rows, local_heads, group, head_size)
    query_pos = own_start + jnp.arange(seq_rows, dtype=jnp.int32)
    gate_query = lax.dynamic_slice_in_dim(cum_gate, own_start, seq_rows, 1)
    gate_rows = jnp.transpose(gate_query)[:, :, None, None]
    scale = head_size ** (-0.5)
    best_start = jnp.full((seq_rows, local_heads, group), -jnp.inf, jnp.float32)
    total_start = jnp.zeros((seq_rows, local_heads, group), jnp.float32)
    summed_start = jnp.zeros((seq_rows, local_heads * group * head_size), jnp.float32)
    pieces = (
        lax.all_gather(key_cache, "ep", axis=2, tiled=True),
        lax.all_gather(value_cache, "ep", axis=2, tiled=True),
    )

    def update(state):
        best, total, summed = state
        key_piece, value_piece = pieces
        width = key_piece.shape[2]
        scores = (
            jnp.einsum("thgd,hds->thgs", query_heads, key_piece, preferred_element_type=jnp.float32)
            * scale
        )
        scores = scores + gate_rows - cum_gate[None, :, None, :]
        key_pos = jnp.arange(width, dtype=jnp.int32)
        allowed = key_pos[None, :] <= query_pos[:, None]
        scores = jnp.where(allowed[:, None, None, :], scores, -jnp.inf)
        new_best = jnp.max(scores, axis=-1)
        factor = jnp.exp(best - new_best)
        weights = jnp.exp(scores - new_best[..., None])
        new_total = total * factor + jnp.sum(weights, axis=-1)
        product = jnp.einsum(
            "thgs,hds->thgd",
            weights.astype(jnp.bfloat16),
            value_piece,
            preferred_element_type=jnp.float32,
        )
        new_summed = summed.reshape(product.shape) * factor[..., None] + product
        return (new_best, new_total, new_summed.reshape(seq_rows, local_heads * group * head_size))

    best, total, summed = lax.cond(
        jnp.int32(0) <= own_start,
        update,
        lambda state: state,
        (best_start, total_start, summed_start),
    )
    attended = summed.reshape(seq_rows, local_heads, group, head_size) / total[..., None]
    attended = attended.astype(jnp.bfloat16).reshape(seq_rows, local_heads * group * head_size)
    by_position = lax.all_to_all(attended, "tp", split_axis=0, concat_axis=1, tiled=True)
    return jnp.dot(by_position, out_weight, preferred_element_type=jnp.float32).astype(jnp.bfloat16)


def expert_half(routed_input, norm_gain, routes, route_weight, expert_gate, expert_up, expert_down):
    group_size = lax.axis_size("tp")
    ep_size = lax.axis_size("ep")
    tp_index = lax.axis_index("tp")
    seq_rows, width = routed_input.shape
    own_rows = seq_rows // group_size
    local_experts = expert_gate.shape[0]
    expert_count = local_experts * ep_size
    top_count = routes.shape[1]
    capacity = max(2, own_rows * top_count * 3 // (2 * expert_count))
    per_device = local_experts * capacity
    mine = lax.dynamic_slice_in_dim(routed_input, tp_index * own_rows, own_rows, 0)
    own_routes = lax.dynamic_slice_in_dim(routes, tp_index * own_rows, own_rows, 0)
    chooser = slot_chooser(own_routes, expert_count, capacity)
    normed = rms_rows(mine, norm_gain)
    outgoing = jnp.einsum("tks,td->sd", chooser, normed, preferred_element_type=jnp.float32).astype(
        jnp.bfloat16
    )
    arrived = lax.all_to_all(
        outgoing.reshape(1, ep_size, per_device, width),
        "ep",
        split_axis=1,
        concat_axis=1,
        tiled=True,
    )
    received = lax.all_gather(arrived, "tp", axis=0, tiled=True)
    blocks = received.shape[0]
    divide_point = received.reshape(blocks, ep_size, local_experts, capacity, width)
    gate = jnp.einsum(
        "abecd,edf->abecf", divide_point, expert_gate, preferred_element_type=jnp.float32
    )
    upper = jnp.einsum(
        "abecd,edf->abecf", divide_point, expert_up, preferred_element_type=jnp.float32
    )
    hidden = (jax.nn.silu(gate) * upper).astype(jnp.bfloat16)
    partial_value = jnp.einsum(
        "abecf,efd->abecd", hidden, expert_down, preferred_element_type=jnp.float32
    )
    rounded = lax.optimization_barrier(partial_value.astype(jnp.bfloat16)).astype(jnp.float32)
    summed = lax.psum_scatter(
        rounded.reshape(lax.axis_size("tp") * 1, ep_size, per_device, width).astype(jnp.bfloat16),
        "tp",
        scatter_dimension=0,
        tiled=True,
    )
    returned = lax.all_to_all(summed, "ep", split_axis=1, concat_axis=1, tiled=True)
    picked = jnp.einsum(
        "tks,sd->tkd",
        chooser,
        returned.reshape(ep_size * per_device, width),
        preferred_element_type=jnp.float32,
    )
    own_weight = lax.dynamic_slice_in_dim(route_weight, tp_index * own_rows, own_rows, 0)
    return jnp.sum(own_weight[:, :, None] * picked, axis=1).astype(jnp.bfloat16)


def body(
    queries,
    key_cache,
    value_cache,
    cum_gate,
    out_weight,
    routed_input,
    norm_gain,
    routes,
    route_weight,
    expert_gate,
    expert_up,
    expert_down,
):
    mixed_out = mixer_half(queries, key_cache, value_cache, cum_gate, out_weight)
    expert_out = expert_half(
        routed_input, norm_gain, routes, route_weight, expert_gate, expert_up, expert_down
    )
    return (mixed_out, expert_out)


def pick_body(
    n,
    tpn,
    queries,
    key_cache,
    value_cache,
    cum_gate,
    out_weight,
    routed_input,
    norm_gain,
    routes,
    route_weight,
    expert_gate,
    *rest,
):
    seq, columns = queries.shape
    own_rows = routed_input.shape[0] // tpn
    cap = block_capacity(own_rows, routes.shape[1], n * expert_gate.shape[0])
    fits = (
        tpn == 4
        and n == 8
        and cap % 8 == 0
        and expert_gate.shape[0] == 1
        and key_cache.shape[0] == 1
        and seq % 128 == 0
    )
    args = (
        queries,
        key_cache,
        value_cache,
        cum_gate,
        out_weight,
        routed_input,
        norm_gain,
        routes,
        route_weight,
        expert_gate,
    ) + rest
    return fused_body(n, tpn, *args) if fits else body(*args)


def solution(mesh):
    return jax.shard_map(
        functools.partial(pick_body, mesh.shape["ep"], mesh.shape["tp"]),
        mesh=mesh,
        in_specs=(
            P("ep", "tp"),
            P("tp", None, "ep"),
            P("tp", None, "ep"),
            P("tp", None),
            P(),
            P("ep", None),
            P(),
            P("ep", None),
            P("ep", None),
            P("ep", None, "tp"),
            P("ep", None, "tp"),
            P("ep", "tp", None),
        ),
        out_specs=(P(("ep", "tp"), None), P(("ep", "tp"), None)),
        check_vma=False,
    )
```

```python
import functools

import jax
import jax.numpy as jnp
from jax import lax
from jax.experimental import pallas as pl
from jax.experimental.pallas import tpu as pltpu
from jax.sharding import PartitionSpec as P

MESH = pl.DeviceIdType.MESH


INNER_SENDS = (2, 7, 1, 5, 4, 6, 3)
OUTER_SENDS = (7, 1, 4, 2, 6, 5, 3)
INNER_STEPS = (
    "C0", "A1", "A6", "C1", "D1", "B6", "A2", "A5", "C6", "E1", "D6", "B5", "C2", "A7",
    "A4", "E6", "C5", "A3", "D5", "C3", "B7", "B4", "D3", "C7", "K", "D7", "C4", "D2",
    "E5", "E3", "D4", "E7", "D0", "T", "E2", "E4", "E0",
)
OUTER_STEPS = (
    "C0", "D0", "A7", "E0", "B7", "A5", "A2", "C7", "A1", "B5", "A6", "D7", "C5", "D5",
    "C1", "B6", "A4", "C6", "E7", "K", "D6", "A3", "E5", "C3", "D1", "B4", "D3", "E6",
    "C2", "C4", "D4", "D2", "E3", "T", "E1", "E4", "E2",
)


def fused_kernel(
    n,
    tpn,
    cap,
    q_any,
    gate_any,
    gain_any,
    routes_any,
    rw_any,
    k_any,
    v_any,
    ow_any,
    x_any,
    wg_any,
    wu_any,
    wd_any,
    mixed_ref,
    out_ref,
    q_ref,
    gate_ref,
    gain_ref,
    routes_ref,
    rw_ref,
    xbuf,
    wgv,
    wuv,
    wdv,
    owv,
    kv,
    att,
    attr,
    sel,
    sbuf,
    sfar,
    recv,
    part,
    r1,
    s2,
    r2,
    s3,
    rbuf,
    lsem,
    kvs,
    kvr,
    ats,
    atr,
    a_s,
    a_r,
    bx_s,
    bx_r,
    f_s,
    f_r,
    r1_s,
    r1_r,
    r2_s,
    r2_r,
    r3_s,
    r3_r,
):
    e = lax.axis_index("ep")
    t = lax.axis_index("tp")
    partner = t + 1 - 2 * lax.rem(t, 2)
    peer = lax.rem(t + 2, tpn)
    opp = lax.rem(partner + 2, tpn)
    mate = e + 1 - 2 * lax.rem(e, 2)
    half = n // 2
    _, own_rows, width = xbuf.shape
    wide = width // 2
    head = k_any.shape[1]
    seq = q_ref.shape[0]

    side = lax.div(e, half)
    base = side * half
    local = lax.rem(e, half)
    row = lax.rem(e, 2)
    inner = lax.div(local, 2) == 1 - side
    rank = jnp.where(inner, 0, 1)

    barrier = pltpu.get_barrier_semaphore()
    for s in range(1, n):
        pl.semaphore_signal(
            barrier, inc=1, device_id={"ep": lax.rem(e + s, n), "tp": t}, device_id_type=MESH
        )
    for s in range(1, tpn):
        pl.semaphore_signal(
            barrier, inc=1, device_id={"ep": e, "tp": lax.rem(t + s, tpn)}, device_id_type=MESH
        )

    blocks = (t, peer, partner, opp)

    def load_x(j):
        at = blocks[j] * own_rows
        return pltpu.make_async_copy(x_any.at[pl.ds(at, own_rows)], xbuf.at[j], lsem.at[12 + j])

    load_k = pltpu.make_async_copy(k_any.at[0], kv.at[e, pl.ds(0, head)], lsem.at[1])
    load_v = pltpu.make_async_copy(v_any.at[0], kv.at[e, pl.ds(head, head)], lsem.at[2])
    load_g = pltpu.make_async_copy(wg_any.at[0], wgv, lsem.at[3])
    load_u = pltpu.make_async_copy(wu_any.at[0], wuv, lsem.at[4])
    load_d = pltpu.make_async_copy(wd_any.at[0], wdv, lsem.at[5])
    load_o = pltpu.make_async_copy(ow_any, owv, lsem.at[6])
    load_q = pltpu.make_async_copy(q_any, q_ref, lsem.at[8])
    load_c = pltpu.make_async_copy(gate_any, gate_ref, lsem.at[9])
    load_n = pltpu.make_async_copy(gain_any, gain_ref, lsem.at[10])
    load_r = pltpu.make_async_copy(routes_any, routes_ref, lsem.at[11])
    load_w = pltpu.make_async_copy(rw_any, rw_ref, lsem.at[0])
    load_r.start()
    load_n.start()
    load_x(0).start()
    load_x(1).start()
    load_k.start()
    load_v.start()
    for j in range(2, tpn):
        load_x(j).start()
    load_g.start()
    load_u.start()
    load_d.start()
    load_w.start()
    load_q.start()
    load_c.start()
    load_o.start()

    def remote(src, dst, ssem, rsem, ep, tp):
        return pltpu.make_async_remote_copy(
            src_ref=src,
            dst_ref=dst,
            send_sem=ssem,
            recv_sem=rsem,
            device_id={"ep": ep, "tp": tp},
            device_id_type=MESH,
        )

    def flip(s):
        s = jnp.int32(s)
        flipped = jnp.int32(0)
        bit = 1
        while bit < n:
            ours = lax.rem(lax.div(e, jnp.int32(bit)), jnp.int32(2))
            theirs = lax.rem(lax.div(s, jnp.int32(bit)), jnp.int32(2))
            flipped = flipped + bit * (ours + theirs - 2 * ours * theirs)
            bit *= 2
        return flipped

    def kv_far(s):
        return remote(kv.at[e], kv.at[e], kvs.at[s], kvr.at[s], lax.rem(e + 2 * s, n), t)

    def kv_far_in(s):
        src = lax.rem(e - 2 * s + n, n)
        return remote(kv.at[src], kv.at[src], kvs.at[s], kvr.at[s], lax.rem(e + 2 * s, n), t)

    def kv_mate(s):
        src = lax.rem(e - 2 * s + n, n)
        return remote(kv.at[src], kv.at[src], kvs.at[half + s], kvr.at[half + s], mate, t)

    def kv_mate_in(s):
        src = lax.rem(mate - 2 * s + n, n)
        return remote(kv.at[src], kv.at[src], kvs.at[half + s], kvr.at[half + s], mate, t)

    def far_sends(s):
        return e + 2 * s < n

    def far_comes(s):
        return e - 2 * s >= 0

    def mate_sends(s):
        return (e - 2 * s >= 0) if s else row == 0

    def mate_comes(s):
        return (mate - 2 * s >= 0) if s else row == 1

    def near(s):
        dst = flip(s)
        return remote(
            sbuf.at[lax.rem(dst, half)],
            recv.at[s, pl.ds(0, 2)],
            a_s.at[s],
            a_r.at[s],
            dst,
            t,
        )

    def far(g):
        dst = source(g)
        mine = half + 2 * rank + g % 2
        return remote(
            sfar.at[lax.rem(dst, half)], recv.at[mine, 0], a_s.at[g], a_r.at[mine], dst, t
        )

    def arrival(g):
        if g < half:
            return remote(sbuf.at[0], recv.at[g, pl.ds(0, 2)], a_s.at[0], a_r.at[g], e, peer)
        return remote(sfar.at[0], recv.at[g, 0], a_s.at[0], a_r.at[g], e, peer)

    def copy_bx(g):
        return remote(recv.at[g, 0], recv.at[g, 1], bx_s.at[g], bx_r.at[g], e, peer)

    def copy_f(g):
        return remote(
            recv.at[g, pl.ds(0, 2)], recv.at[g, pl.ds(2, 2)], f_s.at[g], f_r.at[g], e, partner
        )

    def copy_r1(g):
        return remote(part.at[g, pl.ds(2, 2)], r1.at[g], r1_s.at[g], r1_r.at[g], e, partner)

    def copy_r2(g):
        return remote(s2.at[g], r2.at[g], r2_s.at[g], r2_r.at[g], e, peer)

    def source(g):
        g = jnp.int32(g)
        which = lax.div(g - half, jnp.int32(2))
        turn = lax.rem(g, jnp.int32(2))
        z = jnp.where(side == 0, 2 + which, 1 - which)
        far = 2 * z + row + turn - 2 * row * turn
        return jnp.where(g < half, flip(g), far)

    def copy_r3(g):
        return remote(s3.at[g], rbuf.at[e], r3_s.at[g], r3_r.at[e], source(g), t)

    def copy_r3_in(s):
        src = flip(s)
        return remote(s3.at[0], rbuf.at[src], r3_s.at[0], r3_r.at[src], src, t)

    top, share = routes_ref.shape

    def column(line, block):
        at = block * own_rows
        own = lax.broadcasted_iota(jnp.int32, (own_rows, share), 1) == (
            lax.broadcasted_iota(jnp.int32, (own_rows, share), 0) + at
        )
        return jnp.sum(
            jnp.where(own, jnp.broadcast_to(line, own.shape), 0.0), axis=1, keepdims=True
        )

    def named_by(ref, block):
        return [column(ref[k : k + 1, :].astype(jnp.float32), block) for k in range(top)]

    before = lax.broadcasted_iota(jnp.int32, (own_rows, own_rows), 1) < lax.broadcasted_iota(
        jnp.int32, (own_rows, own_rows), 0
    )

    def lanes_of(first, count):
        lanes = 2 * count * cap
        place = lax.broadcasted_iota(jnp.int32, (own_rows, lanes), 1).astype(jnp.float32) + 0.5
        expert = jnp.floor(place / (2.0 * cap))
        inside = place - 0.5 - expert * (2.0 * cap)
        right = inside >= cap
        slot = jnp.where(right, inside - cap, inside)
        return expert + first.astype(jnp.float32), right, slot

    def hits_of(names, lanes):
        expert, right, slot = lanes
        named = [name == expert for name in names]
        total = sum([m.astype(jnp.float32) for m in named])
        ranks = jnp.dot(
            before.astype(jnp.bfloat16),
            total.astype(jnp.bfloat16),
            preferred_element_type=jnp.float32,
        )
        return named, total, ranks == slot

    def spread_of(names, lanes):
        _, total, hit = hits_of(names, lanes)
        right = lanes[1]
        chosen = jnp.where(hit, total, 0.0)
        spread = jnp.concatenate(
            [jnp.where(right, 0.0, chosen), jnp.where(right, chosen, 0.0)], axis=0
        )
        return spread.T.astype(jnp.bfloat16)

    def chunks(spread, rows):
        return jnp.dot(spread, rows, preferred_element_type=jnp.float32).astype(jnp.bfloat16)

    load_r.wait()
    side_lanes = lanes_of(base, half)
    own_names = named_by(routes_ref, t)
    spread = spread_of(own_names, side_lanes)
    load_n.wait()
    gain = gain_ref[...].astype(jnp.float32)
    gain = jnp.concatenate([gain[j : j + 1, :] for j in range(gain.shape[0])], axis=1)

    def halves(j):
        load_x(j).wait()
        x = xbuf[j].astype(jnp.float32)
        scale = lax.rsqrt(jnp.mean(x * x, axis=-1, keepdims=True) + 1e-06)
        normed = (x * scale * gain).astype(jnp.bfloat16)
        return jnp.concatenate([normed[:, :wide], normed[:, wide:]], axis=0)

    own = halves(0)
    sbuf[:, 0] = chunks(spread, own).reshape(half, 2 * cap, wide)
    sfar[...] = chunks(spread_of(own_names, lanes_of(half - base, half)), own).reshape(sfar.shape)

    with jax.named_scope("barrier"):
        pl.semaphore_wait(barrier, n - 1 + tpn - 1)

    def send(which):
        for g in which:
            (near if g < half else far)(g).start()

    def leading(order):
        return min(p for p, g in enumerate(order) if g < half)

    def by_place(inner_part, outer_part):
        @pl.when(inner)
        def _():
            send(inner_part)

        @pl.when(jnp.logical_not(inner))
        def _():
            send(outer_part)

    inner_first, outer_first = leading(INNER_SENDS), leading(OUTER_SENDS)
    by_place(INNER_SENDS[:inner_first], OUTER_SENDS[:outer_first])
    sbuf[:, 1] = chunks(spread_of(named_by(routes_ref, peer), side_lanes), halves(1)).reshape(
        half, 2 * cap, wide
    )
    by_place(INNER_SENDS[inner_first:], OUTER_SENDS[outer_first:])
    load_k.wait()
    load_v.wait()
    for s in range(1, half):

        @pl.when(far_sends(s))
        def _():
            kv_far(s).start()

    @pl.when(mate_sends(0))
    def _():
        kv_mate(0).start()

    own_lanes = lanes_of(e, 1)
    recv[0, 0:2] = sbuf[local]
    for j in (2, 3):
        recv[0, j] = chunks(spread_of(named_by(routes_ref, blocks[j]), own_lanes), halves(j))

    def copy_att(s):
        dst = lax.rem(t + s, tpn)
        return remote(att.at[dst], attr.at[t], ats.at[s], atr.at[s], e, dst)

    def copy_att_in(s):
        src = lax.rem(t - s + tpn, tpn)
        return remote(att.at[src], attr.at[src], ats.at[s], atr.at[s], e, lax.rem(t + s, tpn))

    def attention():
        for s in range(half):

            @pl.when(mate_comes(s))
            def _():
                kv_mate_in(s).wait_recv()

        for j in range(1, n):

            @pl.when(j > e)
            def _():
                kv[j] = jnp.zeros(kv.shape[1:], kv.dtype)

        load_q.wait()
        load_c.wait()
        own_gate = gate_ref[:, pl.ds(pl.multiple_of(e * seq, seq), seq)]
        eye = lax.broadcasted_iota(jnp.int32, (seq, seq), 0) == lax.broadcasted_iota(
            jnp.int32, (seq, seq), 1
        )
        gate_col = jnp.sum(
            jnp.where(eye, jnp.broadcast_to(own_gate, (seq, seq)), 0.0), axis=1, keepdims=True
        )
        key_pos = lax.broadcasted_iota(jnp.int32, (seq, n * seq), 1)
        query_pos = lax.broadcasted_iota(jnp.int32, (seq, n * seq), 0) + e * seq
        bias = gate_col - gate_ref[...]
        group = q_ref.shape[1] // head
        heads_out = []
        for g in range(group):
            q = q_ref[:, g * head : (g + 1) * head]
            scores = jnp.concatenate(
                [
                    jnp.dot(q, kv[j, 0:head, :], preferred_element_type=jnp.float32)
                    for j in range(n)
                ],
                axis=1,
            )
            scores = scores * (head ** (-0.5)) + bias
            scores = jnp.where(key_pos <= query_pos, scores, -jnp.inf)
            weights = jnp.exp(scores - jnp.max(scores, axis=-1, keepdims=True))
            whole = jnp.sum(weights, axis=-1, keepdims=True)
            weights = weights.astype(jnp.bfloat16)
            summed = jnp.zeros((seq, head), jnp.float32)
            for j in range(n):
                summed = summed + lax.dot_general(
                    weights[:, j * seq : (j + 1) * seq],
                    kv[j, head : 2 * head, :],
                    (((1,), (1,)), ((), ())),
                    preferred_element_type=jnp.float32,
                )
            heads_out.append(summed / whole)
        attended = jnp.concatenate(heads_out, axis=1).astype(jnp.bfloat16)
        att[...] = attended.reshape(att.shape)
        attr[t] = att[t]
        for s in range(1, tpn):
            copy_att(s).start()

    def pass_kv():
        for s in range(1, half):

            @pl.when(far_comes(s))
            def _():
                kv_far_in(s).wait_recv()
                kv_mate(s).start()

    def arrive(g):
        arrival(g).wait_recv()
        (copy_f if g < half else copy_bx)(g).start()

    def spread_pair(g):
        copy_bx(g).wait_recv()
        copy_f(g).start()

    def experts(g):
        if g:
            with jax.named_scope(f"w_f{g}"):
                copy_f(g).wait_recv()
        block = recv[g].astype(jnp.float32)
        count = block.shape[0] * cap
        lo = block[:, :cap].reshape(count, wide).astype(jnp.bfloat16)
        hi = block[:, cap:].reshape(count, wide).astype(jnp.bfloat16)
        gate = jnp.dot(lo, wgv[0:wide, :], preferred_element_type=jnp.float32) + jnp.dot(
            hi, wgv[wide:, :], preferred_element_type=jnp.float32
        )
        upper = jnp.dot(lo, wuv[0:wide, :], preferred_element_type=jnp.float32) + jnp.dot(
            hi, wuv[wide:, :], preferred_element_type=jnp.float32
        )
        hidden = (gate / (1.0 + jnp.exp(-gate)) * upper).astype(jnp.bfloat16)
        down = jnp.dot(hidden, wdv[...], preferred_element_type=jnp.float32)
        shape = (tpn, cap, wide)
        part[g] = jnp.concatenate(
            [down[:, :wide].reshape(shape), down[:, wide:].reshape(shape)], axis=1
        ).astype(jnp.bfloat16)
        copy_r1(g).start()

    def cross(g):
        copy_r1(g).wait_recv()
        s2[g] = (part[g, 1].astype(jnp.float32) + r1[g, 1].astype(jnp.float32)).astype(
            jnp.bfloat16
        )
        copy_r2(g).start()

    def give_back(g):
        copy_r2(g).wait_recv()
        done = (
            part[g, 0].astype(jnp.float32)
            + r1[g, 0].astype(jnp.float32)
            + r2[g].astype(jnp.float32)
        ).astype(jnp.bfloat16)
        if g == 0:
            rbuf[e] = done
        else:
            s3[g] = done
            copy_r3(g).start()

    def first_matmul():
        load_g.wait()
        load_u.wait()
        load_d.wait()

    def choose_back():
        everywhere = lanes_of(e * 0, n)
        named, _, hit = hits_of(own_names, everywhere)
        right = everywhere[1]
        for k in range(top):
            mine = jnp.where(hit & named[k], 1.0, 0.0)
            sel[2 * k * own_rows : (2 * k + 1) * own_rows, :] = jnp.where(
                right, 0.0, mine
            ).astype(jnp.bfloat16)
            sel[(2 * k + 1) * own_rows : (2 * k + 2) * own_rows, :] = jnp.where(
                right, mine, 0.0
            ).astype(jnp.bfloat16)

    kinds = {"A": arrive, "B": spread_pair, "C": experts, "D": cross, "E": give_back}

    def run(steps):
        for name in steps:
            with jax.named_scope(name):
                if name == "K":
                    pass_kv()
                elif name == "T":
                    attention()
                else:
                    kinds[name[0]](int(name[1:]))

    first_matmul()

    @pl.when(inner)
    def _():
        run(INNER_STEPS)

    @pl.when(jnp.logical_not(inner))
    def _():
        run(OUTER_STEPS)

    choose_back()

    with jax.named_scope("w_att"):
        for s in range(1, tpn):
            copy_att_in(s).wait_recv()
        load_o.wait()
    joined = jnp.concatenate([attr[j] for j in range(tpn)], axis=1)
    mixed_ref[...] = jnp.dot(joined, owv[...], preferred_element_type=jnp.float32).astype(
        jnp.bfloat16
    )
    load_w.wait()
    rw = [column(rw_ref[k : k + 1, :], t) for k in range(top)]

    for g in range(1, n):
        (near if g < half else far)(g).wait_send()
    for s in range(1, half):

        @pl.when(far_sends(s))
        def _():
            kv_far(s).wait_send()

    for s in range(half):

        @pl.when(mate_sends(s))
        def _():
            kv_mate(s).wait_send()

    for s in range(1, tpn):
        copy_att(s).wait_send()

    def drain(g, carry):
        @pl.when(g > 0)
        def _():
            copy_f(g).wait_send()

        @pl.when(g >= half)
        def _():
            copy_bx(g).wait_send()

        copy_r1(g).wait_send()
        copy_r2(g).wait_send()
        return carry

    lax.fori_loop(0, n, drain, 0)

    with jax.named_scope("w_r3"):
        for s in range(1, n):
            copy_r3_in(s).wait_recv()
    lanes = 2 * n * cap
    picked = jnp.dot(
        sel[...], rbuf[...].reshape(lanes, wide), preferred_element_type=jnp.float32
    )
    for h in range(2):
        acc = jnp.zeros((own_rows, wide), jnp.float32)
        for k in range(top):
            at = (2 * k + h) * own_rows
            acc = acc + rw[k] * picked[at : at + own_rows]
        out_ref[:, h * wide : (h + 1) * wide] = acc.astype(jnp.bfloat16)

    def last(g, carry):
        copy_r3(g).wait_send()
        return carry

    lax.fori_loop(1, n, last, 0)


def fused_body(
    n,
    tpn,
    queries,
    key_cache,
    value_cache,
    cum_gate,
    out_weight,
    routed_input,
    norm_gain,
    routes,
    route_weight,
    expert_gate,
    expert_up,
    expert_down,
):
    seq = queries.shape[0]
    head = key_cache.shape[1]
    width = routed_input.shape[1]
    wide = width // 2
    own_rows = routed_input.shape[0] // tpn
    top = routes.shape[1]
    units = expert_gate.shape[2]
    cap = block_capacity(own_rows, top, n * expert_gate.shape[0])
    half = n // 2
    bf16 = jnp.bfloat16
    chunk = (2 * cap, wide)
    anywhere = pl.BlockSpec(memory_space=pltpu.HBM)
    vmem = pl.BlockSpec(memory_space=pltpu.VMEM)
    dma = pltpu.SemaphoreType.DMA
    mixed, out = pl.pallas_call(
        functools.partial(fused_kernel, n, tpn, cap),
        out_shape=(
            pltpu.VMEM((seq // tpn, width), bf16),
            pltpu.VMEM((own_rows, width), bf16),
        ),
        in_specs=[anywhere] * 12,
        out_specs=(vmem, vmem),
        scratch_shapes=[
            pltpu.VMEM(queries.shape, bf16),
            pltpu.VMEM(cum_gate.shape, jnp.float32),
            pltpu.VMEM((width // 128, 128), bf16),
            pltpu.VMEM((top, tpn * own_rows), jnp.int32),
            pltpu.VMEM((top, tpn * own_rows), jnp.float32),
            pltpu.VMEM((tpn, own_rows, width), bf16),
            pltpu.VMEM((width, units), bf16),
            pltpu.VMEM((width, units), bf16),
            pltpu.VMEM((units, width), bf16),
            pltpu.VMEM(out_weight.shape, bf16),
            pltpu.VMEM((n, 2 * head, seq), bf16),
            pltpu.VMEM((tpn, seq // tpn, queries.shape[1]), bf16),
            pltpu.VMEM((tpn, seq // tpn, queries.shape[1]), bf16),
            pltpu.VMEM((2 * top * own_rows, 2 * n * cap), bf16),
            pltpu.VMEM((half, 2) + chunk, bf16),
            pltpu.VMEM((half,) + chunk, bf16),
            pltpu.VMEM((n, tpn) + chunk, bf16),
            pltpu.VMEM((n, tpn) + chunk, bf16),
            pltpu.VMEM((n, 2) + chunk, bf16),
            pltpu.VMEM((n,) + chunk, bf16),
            pltpu.VMEM((n,) + chunk, bf16),
            pltpu.VMEM((n,) + chunk, bf16),
            pltpu.VMEM((n,) + chunk, bf16),
            dma((12 + tpn,)),
            dma((n,)),
            dma((n,)),
            dma((tpn,)),
            dma((tpn,)),
        ]
        + [dma((n,))] * 12,
        compiler_params=pltpu.CompilerParams(
            collective_id=0, has_side_effects=True, vmem_limit_bytes=60 * 1024 * 1024
        ),
    )(
        queries,
        cum_gate,
        norm_gain.reshape(width // 128, 128),
        routes.T,
        route_weight.T,
        key_cache,
        value_cache,
        out_weight,
        routed_input,
        expert_gate,
        expert_up,
        expert_down,
    )
    return write_out(mixed, out)


def write_kernel(a, b, a_out, b_out, sem):
    copies = [
        pltpu.make_async_copy(a, a_out, sem.at[0]),
        pltpu.make_async_copy(b, b_out, sem.at[1]),
    ]
    for copy in copies:
        copy.start()
    for copy in copies:
        copy.wait()


def write_out(*arrays):
    return pl.pallas_call(
        write_kernel,
        out_shape=[jax.ShapeDtypeStruct(a.shape, a.dtype) for a in arrays],
        in_specs=[pl.BlockSpec(memory_space=pltpu.VMEM)] * len(arrays),
        out_specs=[pl.BlockSpec(memory_space=pltpu.HBM)] * len(arrays),
        scratch_shapes=[pltpu.SemaphoreType.DMA((len(arrays),))],
    )(*[pltpu.with_memory_space_constraint(a, pltpu.VMEM) for a in arrays])


def block_capacity(own_rows, top_count, expert_count):
    return max(2, own_rows * top_count * 3 // (2 * expert_count))


def slot_chooser(route_rows, expert_count, capacity):
    token_rows, top_count = route_rows.shape
    flat = route_rows.reshape(token_rows * top_count)
    same = (flat[:, None] == jnp.arange(expert_count, dtype=jnp.int32)[None, :]).astype(jnp.int32)
    earlier = jnp.cumsum(same, axis=0) - same
    rank = jnp.sum(earlier * same, axis=1)
    slot = flat * capacity + rank
    chosen = slot[:, None] == jnp.arange(expert_count * capacity, dtype=jnp.int32)[None, :]
    return chosen.astype(jnp.bfloat16).reshape(token_rows, top_count, expert_count * capacity)


def rms_rows(source, norm_gain):
    widened = source.astype(jnp.float32)
    scale = lax.rsqrt(jnp.mean(widened * widened, axis=-1, keepdims=True) + 1e-06)
    return (widened * scale * norm_gain.astype(jnp.float32)).astype(jnp.bfloat16)


def mixer_half(queries, key_cache, value_cache, cum_gate, out_weight):
    seq_rows = queries.shape[0]
    local_heads = key_cache.shape[0]
    head_size = key_cache.shape[1]
    group = queries.shape[1] // (local_heads * head_size)
    own_start = lax.axis_index("ep") * seq_rows
    query_heads = queries.reshape(seq_rows, local_heads, group, head_size)
    query_pos = own_start + jnp.arange(seq_rows, dtype=jnp.int32)
    gate_query = lax.dynamic_slice_in_dim(cum_gate, own_start, seq_rows, 1)
    gate_rows = jnp.transpose(gate_query)[:, :, None, None]
    scale = head_size ** (-0.5)
    best_start = jnp.full((seq_rows, local_heads, group), -jnp.inf, jnp.float32)
    total_start = jnp.zeros((seq_rows, local_heads, group), jnp.float32)
    summed_start = jnp.zeros((seq_rows, local_heads * group * head_size), jnp.float32)
    pieces = (
        lax.all_gather(key_cache, "ep", axis=2, tiled=True),
        lax.all_gather(value_cache, "ep", axis=2, tiled=True),
    )

    def update(state):
        best, total, summed = state
        key_piece, value_piece = pieces
        width = key_piece.shape[2]
        scores = (
            jnp.einsum("thgd,hds->thgs", query_heads, key_piece, preferred_element_type=jnp.float32)
            * scale
        )
        scores = scores + gate_rows - cum_gate[None, :, None, :]
        key_pos = jnp.arange(width, dtype=jnp.int32)
        allowed = key_pos[None, :] <= query_pos[:, None]
        scores = jnp.where(allowed[:, None, None, :], scores, -jnp.inf)
        new_best = jnp.max(scores, axis=-1)
        factor = jnp.exp(best - new_best)
        weights = jnp.exp(scores - new_best[..., None])
        new_total = total * factor + jnp.sum(weights, axis=-1)
        product = jnp.einsum(
            "thgs,hds->thgd",
            weights.astype(jnp.bfloat16),
            value_piece,
            preferred_element_type=jnp.float32,
        )
        new_summed = summed.reshape(product.shape) * factor[..., None] + product
        return (new_best, new_total, new_summed.reshape(seq_rows, local_heads * group * head_size))

    best, total, summed = lax.cond(
        jnp.int32(0) <= own_start,
        update,
        lambda state: state,
        (best_start, total_start, summed_start),
    )
    attended = summed.reshape(seq_rows, local_heads, group, head_size) / total[..., None]
    attended = attended.astype(jnp.bfloat16).reshape(seq_rows, local_heads * group * head_size)
    by_position = lax.all_to_all(attended, "tp", split_axis=0, concat_axis=1, tiled=True)
    return jnp.dot(by_position, out_weight, preferred_element_type=jnp.float32).astype(jnp.bfloat16)


def expert_half(routed_input, norm_gain, routes, route_weight, expert_gate, expert_up, expert_down):
    group_size = lax.axis_size("tp")
    ep_size = lax.axis_size("ep")
    tp_index = lax.axis_index("tp")
    seq_rows, width = routed_input.shape
    own_rows = seq_rows // group_size
    local_experts = expert_gate.shape[0]
    expert_count = local_experts * ep_size
    top_count = routes.shape[1]
    capacity = max(2, own_rows * top_count * 3 // (2 * expert_count))
    per_device = local_experts * capacity
    mine = lax.dynamic_slice_in_dim(routed_input, tp_index * own_rows, own_rows, 0)
    own_routes = lax.dynamic_slice_in_dim(routes, tp_index * own_rows, own_rows, 0)
    chooser = slot_chooser(own_routes, expert_count, capacity)
    normed = rms_rows(mine, norm_gain)
    outgoing = jnp.einsum("tks,td->sd", chooser, normed, preferred_element_type=jnp.float32).astype(
        jnp.bfloat16
    )
    arrived = lax.all_to_all(
        outgoing.reshape(1, ep_size, per_device, width),
        "ep",
        split_axis=1,
        concat_axis=1,
        tiled=True,
    )
    received = lax.all_gather(arrived, "tp", axis=0, tiled=True)
    blocks = received.shape[0]
    divide_point = received.reshape(blocks, ep_size, local_experts, capacity, width)
    gate = jnp.einsum(
        "abecd,edf->abecf", divide_point, expert_gate, preferred_element_type=jnp.float32
    )
    upper = jnp.einsum(
        "abecd,edf->abecf", divide_point, expert_up, preferred_element_type=jnp.float32
    )
    hidden = (jax.nn.silu(gate) * upper).astype(jnp.bfloat16)
    partial_value = jnp.einsum(
        "abecf,efd->abecd", hidden, expert_down, preferred_element_type=jnp.float32
    )
    rounded = lax.optimization_barrier(partial_value.astype(jnp.bfloat16)).astype(jnp.float32)
    summed = lax.psum_scatter(
        rounded.reshape(lax.axis_size("tp") * 1, ep_size, per_device, width).astype(jnp.bfloat16),
        "tp",
        scatter_dimension=0,
        tiled=True,
    )
    returned = lax.all_to_all(summed, "ep", split_axis=1, concat_axis=1, tiled=True)
    picked = jnp.einsum(
        "tks,sd->tkd",
        chooser,
        returned.reshape(ep_size * per_device, width),
        preferred_element_type=jnp.float32,
    )
    own_weight = lax.dynamic_slice_in_dim(route_weight, tp_index * own_rows, own_rows, 0)
    return jnp.sum(own_weight[:, :, None] * picked, axis=1).astype(jnp.bfloat16)


def body(
    queries,
    key_cache,
    value_cache,
    cum_gate,
    out_weight,
    routed_input,
    norm_gain,
    routes,
    route_weight,
    expert_gate,
    expert_up,
    expert_down,
):
    mixed_out = mixer_half(queries, key_cache, value_cache, cum_gate, out_weight)
    expert_out = expert_half(
        routed_input, norm_gain, routes, route_weight, expert_gate, expert_up, expert_down
    )
    return (mixed_out, expert_out)


def pick_body(
    n,
    tpn,
    queries,
    key_cache,
    value_cache,
    cum_gate,
    out_weight,
    routed_input,
    norm_gain,
    routes,
    route_weight,
    expert_gate,
    *rest,
):
    seq, columns = queries.shape
    own_rows = routed_input.shape[0] // tpn
    cap = block_capacity(own_rows, routes.shape[1], n * expert_gate.shape[0])
    fits = (
        tpn == 4
        and n == 8
        and cap % 8 == 0
        and expert_gate.shape[0] == 1
        and key_cache.shape[0] == 1
        and seq % 128 == 0
    )
    args = (
        queries,
        key_cache,
        value_cache,
        cum_gate,
        out_weight,
        routed_input,
        norm_gain,
        routes,
        route_weight,
        expert_gate,
    ) + rest
    return fused_body(n, tpn, *args) if fits else body(*args)


def solution(mesh):
    return jax.shard_map(
        functools.partial(pick_body, mesh.shape["ep"], mesh.shape["tp"]),
        mesh=mesh,
        in_specs=(
            P("ep", "tp"),
            P("tp", None, "ep"),
            P("tp", None, "ep"),
            P("tp", None),
            P(),
            P("ep", None),
            P(),
            P("ep", None),
            P("ep", None),
            P("ep", None, "tp"),
            P("ep", None, "tp"),
            P("ep", "tp", None),
        ),
        out_specs=(P(("ep", "tp"), None), P(("ep", "tp"), None)),
        check_vma=False,
    )
```

```python
import functools

import jax
import jax.numpy as jnp
from jax import lax
from jax.experimental import pallas as pl
from jax.experimental.pallas import tpu as pltpu
from jax.sharding import PartitionSpec as P

MESH = pl.DeviceIdType.MESH


INNER_SENDS = (1, 2, 3, 6, 5, 7, 4)
OUTER_SENDS = (4, 2, 7, 5, 1, 6, 3)
INNER_STEPS = (
    "C0", "D0", "A6", "E0", "B6", "A2", "A5", "C2", "D2", "A7", "C6", "B5", "D6", "C5",
    "D5", "E2", "B7", "C7", "E6", "A1", "A4", "A3", "C3", "E5", "D7", "C1", "D1", "B4",
    "K", "D3", "C4", "E7", "D4", "E1", "E3", "E4", "T",
)
OUTER_STEPS = (
    "C0", "D0", "A4", "A1", "E0", "C1", "D1", "B4", "A7", "C4", "D4", "E1", "A6", "A2",
    "B7", "E4", "A5", "C7", "A3", "C2", "D7", "B6", "C3", "D3", "K", "C6", "B5", "E7",
    "D6", "C5", "E3", "D5", "E6", "D2", "T", "E5", "E2",
)


def fused_kernel(
    n,
    tpn,
    cap,
    q_any,
    gate_any,
    gain_any,
    routes_any,
    rw_any,
    k_any,
    v_any,
    ow_any,
    x_any,
    wg_any,
    wu_any,
    wd_any,
    mixed_ref,
    out_ref,
    q_ref,
    gate_ref,
    gain_ref,
    routes_ref,
    rw_ref,
    xbuf,
    wgv,
    wuv,
    wdv,
    owv,
    kv,
    att,
    attr,
    sel,
    sbuf,
    sfar,
    recv,
    part,
    r1,
    s2,
    r2,
    s3,
    rbuf,
    lsem,
    kvs,
    kvr,
    sent,
    a_r,
    bx_r,
    f_r,
    r1_r,
    r2_r,
    all_r,
):
    e = lax.axis_index("ep")
    t = lax.axis_index("tp")
    partner = t + 1 - 2 * lax.rem(t, 2)
    peer = lax.rem(t + 2, tpn)
    opp = lax.rem(partner + 2, tpn)
    mate = e + 1 - 2 * lax.rem(e, 2)
    half = n // 2
    _, own_rows, width = xbuf.shape
    wide = width // 2
    head = k_any.shape[1]
    seq = q_ref.shape[0]

    side = lax.div(e, half)
    base = side * half
    local = lax.rem(e, half)
    row = lax.rem(e, 2)
    inner = lax.div(local, 2) == 1 - side
    rank = jnp.where(inner, 0, 1)

    barrier = pltpu.get_barrier_semaphore()
    for s in range(1, n):
        pl.semaphore_signal(
            barrier, inc=1, device_id={"ep": lax.rem(e + s, n), "tp": t}, device_id_type=MESH
        )
    for s in range(1, tpn):
        pl.semaphore_signal(
            barrier, inc=1, device_id={"ep": e, "tp": lax.rem(t + s, tpn)}, device_id_type=MESH
        )

    blocks = (t, peer, partner, opp)

    def load_x(j):
        at = blocks[j] * own_rows
        return pltpu.make_async_copy(x_any.at[pl.ds(at, own_rows)], xbuf.at[j], lsem.at[12 + j])

    load_k = pltpu.make_async_copy(k_any.at[0], kv.at[e, pl.ds(0, head)], lsem.at[1])
    load_v = pltpu.make_async_copy(v_any.at[0], kv.at[e, pl.ds(head, head)], lsem.at[2])
    load_g = pltpu.make_async_copy(wg_any.at[0], wgv, lsem.at[3])
    load_u = pltpu.make_async_copy(wu_any.at[0], wuv, lsem.at[4])
    load_d = pltpu.make_async_copy(wd_any.at[0], wdv, lsem.at[5])
    load_o = pltpu.make_async_copy(ow_any, owv, lsem.at[6])
    load_q = pltpu.make_async_copy(q_any, q_ref, lsem.at[8])
    load_c = pltpu.make_async_copy(gate_any, gate_ref, lsem.at[9])
    load_n = pltpu.make_async_copy(gain_any, gain_ref, lsem.at[10])
    load_r = pltpu.make_async_copy(routes_any, routes_ref, lsem.at[11])
    load_w = pltpu.make_async_copy(rw_any, rw_ref, lsem.at[0])
    load_r.start()
    load_n.start()
    load_x(0).start()
    load_x(1).start()
    load_k.start()
    load_v.start()
    for j in range(2, tpn):
        load_x(j).start()
    load_g.start()
    load_u.start()
    load_d.start()
    load_w.start()
    load_q.start()
    load_c.start()
    load_o.start()

    def remote(src, dst, ssem, rsem, ep, tp):
        return pltpu.make_async_remote_copy(
            src_ref=src,
            dst_ref=dst,
            send_sem=ssem,
            recv_sem=rsem,
            device_id={"ep": ep, "tp": tp},
            device_id_type=MESH,
        )

    def flip(s):
        s = jnp.int32(s)
        flipped = jnp.int32(0)
        bit = 1
        while bit < n:
            ours = lax.rem(lax.div(e, jnp.int32(bit)), jnp.int32(2))
            theirs = lax.rem(lax.div(s, jnp.int32(bit)), jnp.int32(2))
            flipped = flipped + bit * (ours + theirs - 2 * ours * theirs)
            bit *= 2
        return flipped

    def kv_far(s):
        return remote(kv.at[e], kv.at[e], kvs.at[s], kvr.at[s], lax.rem(e + 2 * s, n), t)

    def kv_far_in(s):
        src = lax.rem(e - 2 * s + n, n)
        return remote(kv.at[src], kv.at[src], kvs.at[s], kvr.at[s], lax.rem(e + 2 * s, n), t)

    def kv_mate(s):
        src = lax.rem(e - 2 * s + n, n)
        return remote(kv.at[src], kv.at[src], kvs.at[half + s], kvr.at[half + s], mate, t)

    def kv_mate_in(s):
        src = lax.rem(mate - 2 * s + n, n)
        return remote(kv.at[src], kv.at[src], kvs.at[half + s], kvr.at[half + s], mate, t)

    def far_sends(s):
        return e + 2 * s < n

    def far_comes(s):
        return e - 2 * s >= 0

    def mate_sends(s):
        return (e - 2 * s >= 0) if s else row == 0

    def mate_comes(s):
        return (mate - 2 * s >= 0) if s else row == 1

    def near(s):
        dst = flip(s)
        return remote(
            sbuf.at[lax.rem(dst, half)],
            recv.at[s, pl.ds(0, 2)],
            sent.at[0],
            a_r.at[s],
            dst,
            t,
        )

    def far(g):
        dst = source(g)
        mine = half + 2 * rank + g % 2
        return remote(
            sfar.at[lax.rem(dst, half)], recv.at[mine, 0], sent.at[0], a_r.at[mine], dst, t
        )

    def arrival(g):
        if g < half:
            return remote(sbuf.at[0], recv.at[g, pl.ds(0, 2)], sent.at[0], a_r.at[g], e, peer)
        return remote(sfar.at[0], recv.at[g, 0], sent.at[0], a_r.at[g], e, peer)

    def copy_bx(g):
        return remote(recv.at[g, 0], recv.at[g, 1], sent.at[1], bx_r.at[g - half], e, peer)

    def copy_f(g):
        return remote(
            recv.at[g, pl.ds(0, 2)], recv.at[g, pl.ds(2, 2)], sent.at[2], f_r.at[g], e, partner
        )

    def copy_r1(g):
        return remote(part.at[g, pl.ds(2, 2)], r1.at[g], sent.at[3], r1_r.at[g], e, partner)

    def copy_r2(g):
        return remote(s2.at[g], r2.at[g], sent.at[4], r2_r.at[g], e, peer)

    def source(g):
        g = jnp.int32(g)
        which = lax.div(g - half, jnp.int32(2))
        turn = lax.rem(g, jnp.int32(2))
        z = jnp.where(side == 0, 2 + which, 1 - which)
        far = 2 * z + row + turn - 2 * row * turn
        return jnp.where(g < half, flip(g), far)

    def copy_r3(g):
        return remote(s3.at[g], rbuf.at[e], sent.at[5], all_r.at[0], source(g), t)

    top, share = routes_ref.shape

    def column(line, block):
        at = block * own_rows
        own = lax.broadcasted_iota(jnp.int32, (own_rows, share), 1) == (
            lax.broadcasted_iota(jnp.int32, (own_rows, share), 0) + at
        )
        return jnp.sum(
            jnp.where(own, jnp.broadcast_to(line, own.shape), 0.0), axis=1, keepdims=True
        )

    def named_by(ref, block):
        return [column(ref[k : k + 1, :].astype(jnp.float32), block) for k in range(top)]

    before = lax.broadcasted_iota(jnp.int32, (own_rows, own_rows), 1) < lax.broadcasted_iota(
        jnp.int32, (own_rows, own_rows), 0
    )

    def lanes_of(first, count):
        lanes = 2 * count * cap
        place = lax.broadcasted_iota(jnp.int32, (own_rows, lanes), 1).astype(jnp.float32) + 0.5
        expert = jnp.floor(place / (2.0 * cap))
        inside = place - 0.5 - expert * (2.0 * cap)
        right = inside >= cap
        slot = jnp.where(right, inside - cap, inside)
        return expert + first.astype(jnp.float32), right, slot

    def hits_of(names, lanes):
        expert, right, slot = lanes
        named = [name == expert for name in names]
        total = sum([m.astype(jnp.float32) for m in named])
        ranks = jnp.dot(
            before.astype(jnp.bfloat16),
            total.astype(jnp.bfloat16),
            preferred_element_type=jnp.float32,
        )
        return named, total, ranks == slot

    def spread_of(names, lanes):
        _, total, hit = hits_of(names, lanes)
        right = lanes[1]
        chosen = jnp.where(hit, total, 0.0)
        spread = jnp.concatenate(
            [jnp.where(right, 0.0, chosen), jnp.where(right, chosen, 0.0)], axis=0
        )
        return spread.T.astype(jnp.bfloat16)

    def chunks(spread, rows):
        return jnp.dot(spread, rows, preferred_element_type=jnp.float32).astype(jnp.bfloat16)

    with jax.named_scope("w_r"):
        load_r.wait()
    side_lanes = lanes_of(base, half)
    own_names = named_by(routes_ref, t)
    spread = spread_of(own_names, side_lanes)
    load_n.wait()
    gain = gain_ref[...].astype(jnp.float32)
    gain = jnp.concatenate([gain[j : j + 1, :] for j in range(gain.shape[0])], axis=1)

    def halves(j):
        with jax.named_scope(f"w_x{j}"):
            load_x(j).wait()
        x = xbuf[j].astype(jnp.float32)
        scale = lax.rsqrt(jnp.mean(x * x, axis=-1, keepdims=True) + 1e-06)
        normed = (x * scale * gain).astype(jnp.bfloat16)
        return jnp.concatenate([normed[:, :wide], normed[:, wide:]], axis=0)

    own = halves(0)
    sbuf[:, 0] = chunks(spread, own).reshape(half, 2 * cap, wide)
    sfar[...] = chunks(spread_of(own_names, lanes_of(half - base, half)), own).reshape(sfar.shape)

    sbuf[:, 1] = chunks(spread_of(named_by(routes_ref, peer), side_lanes), halves(1)).reshape(
        half, 2 * cap, wide
    )

    with jax.named_scope("barrier"):
        pl.semaphore_wait(barrier, n - 1 + tpn - 1)

    def send(which):
        for g in which:
            (near if g < half else far)(g).start()

    def by_place(inner_part, outer_part):
        @pl.when(inner)
        def _():
            send(inner_part)

        @pl.when(jnp.logical_not(inner))
        def _():
            send(outer_part)

    by_place(INNER_SENDS, OUTER_SENDS)
    load_k.wait()
    load_v.wait()
    for s in range(1, half):

        @pl.when(far_sends(s))
        def _():
            kv_far(s).start()

    @pl.when(mate_sends(0))
    def _():
        kv_mate(0).start()

    own_lanes = lanes_of(e, 1)
    recv[0, 0:2] = sbuf[local]
    for j in (2, 3):
        recv[0, j] = chunks(spread_of(named_by(routes_ref, blocks[j]), own_lanes), halves(j))

    def copy_att(s):
        dst = lax.rem(t + s, tpn)
        return remote(att.at[dst], attr.at[t], sent.at[6], all_r.at[1], e, dst)

    def joint(ref, ssem, rsem):
        return remote(ref, ref, ssem, rsem, e, peer)

    att_joint = joint(attr.at[pl.ds(0, tpn - 1)], sent.at[6], all_r.at[1])

    def attention():
        for s in range(half):

            @pl.when(mate_comes(s))
            def _():
                kv_mate_in(s).wait_recv()

        for j in range(1, n):

            @pl.when(j > e)
            def _():
                kv[j] = jnp.zeros(kv.shape[1:], kv.dtype)

        load_q.wait()
        load_c.wait()
        own_gate = gate_ref[:, pl.ds(pl.multiple_of(e * seq, seq), seq)]
        eye = lax.broadcasted_iota(jnp.int32, (seq, seq), 0) == lax.broadcasted_iota(
            jnp.int32, (seq, seq), 1
        )
        gate_col = jnp.sum(
            jnp.where(eye, jnp.broadcast_to(own_gate, (seq, seq)), 0.0), axis=1, keepdims=True
        )
        key_pos = lax.broadcasted_iota(jnp.int32, (seq, n * seq), 1)
        query_pos = lax.broadcasted_iota(jnp.int32, (seq, n * seq), 0) + e * seq
        bias = gate_col - gate_ref[...]
        group = q_ref.shape[1] // head
        heads_out = []
        for g in range(group):
            q = q_ref[:, g * head : (g + 1) * head]
            scores = jnp.concatenate(
                [
                    jnp.dot(q, kv[j, 0:head, :], preferred_element_type=jnp.float32)
                    for j in range(n)
                ],
                axis=1,
            )
            scores = scores * (head ** (-0.5)) + bias
            scores = jnp.where(key_pos <= query_pos, scores, -jnp.inf)
            weights = jnp.exp(scores - jnp.max(scores, axis=-1, keepdims=True))
            whole = jnp.sum(weights, axis=-1, keepdims=True)
            weights = weights.astype(jnp.bfloat16)
            summed = jnp.zeros((seq, head), jnp.float32)
            for j in range(n):
                summed = summed + lax.dot_general(
                    weights[:, j * seq : (j + 1) * seq],
                    kv[j, head : 2 * head, :],
                    (((1,), (1,)), ((), ())),
                    preferred_element_type=jnp.float32,
                )
            heads_out.append(summed / whole)
        attended = jnp.concatenate(heads_out, axis=1).astype(jnp.bfloat16)
        att[...] = attended.reshape(att.shape)
        attr[t] = att[t]
        for s in range(1, tpn):
            copy_att(s).start()

    def pass_kv():
        for s in range(1, half):

            @pl.when(far_comes(s))
            def _():
                kv_far_in(s).wait_recv()
                kv_mate(s).start()

    def arrive(g):
        arrival(g).wait_recv()
        (copy_f if g < half else copy_bx)(g).start()

    def spread_pair(g):
        copy_bx(g).wait_recv()
        copy_f(g).start()

    def experts(g):
        if g:
            with jax.named_scope(f"w_f{g}"):
                copy_f(g).wait_recv()
        block = recv[g].astype(jnp.float32)
        count = block.shape[0] * cap
        lo = block[:, :cap].reshape(count, wide).astype(jnp.bfloat16)
        hi = block[:, cap:].reshape(count, wide).astype(jnp.bfloat16)
        gate = jnp.dot(lo, wgv[0:wide, :], preferred_element_type=jnp.float32) + jnp.dot(
            hi, wgv[wide:, :], preferred_element_type=jnp.float32
        )
        upper = jnp.dot(lo, wuv[0:wide, :], preferred_element_type=jnp.float32) + jnp.dot(
            hi, wuv[wide:, :], preferred_element_type=jnp.float32
        )
        hidden = (gate / (1.0 + jnp.exp(-gate)) * upper).astype(jnp.bfloat16)
        down = jnp.dot(hidden, wdv[...], preferred_element_type=jnp.float32)
        shape = (tpn, cap, wide)
        part[g] = jnp.concatenate(
            [down[:, :wide].reshape(shape), down[:, wide:].reshape(shape)], axis=1
        ).astype(jnp.bfloat16)
        copy_r1(g).start()

    def cross(g):
        copy_r1(g).wait_recv()
        s2[g] = (part[g, 1].astype(jnp.float32) + r1[g, 1].astype(jnp.float32)).astype(
            jnp.bfloat16
        )
        copy_r2(g).start()

    def give_back(g):
        copy_r2(g).wait_recv()
        done = (
            part[g, 0].astype(jnp.float32)
            + r1[g, 0].astype(jnp.float32)
            + r2[g].astype(jnp.float32)
        ).astype(jnp.bfloat16)
        if g == 0:
            rbuf[e] = done
        else:
            s3[g] = done
            copy_r3(g).start()

    def first_matmul():
        load_g.wait()
        load_u.wait()
        load_d.wait()

    def choose_back():
        everywhere = lanes_of(e * 0, n)
        named, _, hit = hits_of(own_names, everywhere)
        right = everywhere[1]
        for k in range(top):
            mine = jnp.where(hit & named[k], 1.0, 0.0)
            sel[2 * k * own_rows : (2 * k + 1) * own_rows, :] = jnp.where(
                right, 0.0, mine
            ).astype(jnp.bfloat16)
            sel[(2 * k + 1) * own_rows : (2 * k + 2) * own_rows, :] = jnp.where(
                right, mine, 0.0
            ).astype(jnp.bfloat16)

    kinds = {"A": arrive, "B": spread_pair, "C": experts, "D": cross, "E": give_back}

    def run(steps):
        for name in steps:
            with jax.named_scope(name):
                if name == "K":
                    pass_kv()
                elif name == "T":
                    attention()
                else:
                    kinds[name[0]](int(name[1:]))

    first_matmul()

    @pl.when(inner)
    def _():
        run(INNER_STEPS)

    @pl.when(jnp.logical_not(inner))
    def _():
        run(OUTER_STEPS)

    choose_back()

    with jax.named_scope("w_att"):
        att_joint.wait_recv()
        load_o.wait()
    joined = jnp.concatenate([attr[j] for j in range(tpn)], axis=1)
    mixed_ref[...] = jnp.dot(joined, owv[...], preferred_element_type=jnp.float32).astype(
        jnp.bfloat16
    )
    load_w.wait()
    rw = [column(rw_ref[k : k + 1, :], t) for k in range(top)]

    fives = recv.at[pl.ds(0, half + 1), pl.ds(0, 2)]
    for which, ref in enumerate(
        (
            fives,
            recv.at[pl.ds(half, half), 0],
            recv.at[pl.ds(1, n - 1), pl.ds(0, 2)],
            part.at[:, pl.ds(2, 2)],
            s2,
        )
    ):
        joint(ref, sent.at[which], all_r.at[0]).wait_send()
    for s in range(1, half):

        @pl.when(far_sends(s))
        def _():
            kv_far(s).wait_send()

    for s in range(half):

        @pl.when(mate_sends(s))
        def _():
            kv_mate(s).wait_send()

    att_joint.wait_send()

    with jax.named_scope("w_r3"):
        joint(rbuf.at[pl.ds(0, n - 1)], sent.at[5], all_r.at[0]).wait_recv()
    lanes = 2 * n * cap
    picked = jnp.dot(
        sel[...], rbuf[...].reshape(lanes, wide), preferred_element_type=jnp.float32
    )
    for h in range(2):
        acc = jnp.zeros((own_rows, wide), jnp.float32)
        for k in range(top):
            at = (2 * k + h) * own_rows
            acc = acc + rw[k] * picked[at : at + own_rows]
        out_ref[:, h * wide : (h + 1) * wide] = acc.astype(jnp.bfloat16)

    joint(s3.at[pl.ds(1, n - 1)], sent.at[5], all_r.at[0]).wait_send()


def fused_body(
    n,
    tpn,
    queries,
    key_cache,
    value_cache,
    cum_gate,
    out_weight,
    routed_input,
    norm_gain,
    routes,
    route_weight,
    expert_gate,
    expert_up,
    expert_down,
):
    seq = queries.shape[0]
    head = key_cache.shape[1]
    width = routed_input.shape[1]
    wide = width // 2
    own_rows = routed_input.shape[0] // tpn
    top = routes.shape[1]
    units = expert_gate.shape[2]
    cap = block_capacity(own_rows, top, n * expert_gate.shape[0])
    half = n // 2
    bf16 = jnp.bfloat16
    chunk = (2 * cap, wide)
    anywhere = pl.BlockSpec(memory_space=pltpu.HBM)
    vmem = pl.BlockSpec(memory_space=pltpu.VMEM)
    dma = pltpu.SemaphoreType.DMA
    mixed, out = pl.pallas_call(
        functools.partial(fused_kernel, n, tpn, cap),
        out_shape=(
            pltpu.VMEM((seq // tpn, width), bf16),
            pltpu.VMEM((own_rows, width), bf16),
        ),
        in_specs=[anywhere] * 12,
        out_specs=(vmem, vmem),
        scratch_shapes=[
            pltpu.VMEM(queries.shape, bf16),
            pltpu.VMEM(cum_gate.shape, jnp.float32),
            pltpu.VMEM((width // 128, 128), bf16),
            pltpu.VMEM((top, tpn * own_rows), jnp.int32),
            pltpu.VMEM((top, tpn * own_rows), jnp.float32),
            pltpu.VMEM((tpn, own_rows, width), bf16),
            pltpu.VMEM((width, units), bf16),
            pltpu.VMEM((width, units), bf16),
            pltpu.VMEM((units, width), bf16),
            pltpu.VMEM(out_weight.shape, bf16),
            pltpu.VMEM((n, 2 * head, seq), bf16),
            pltpu.VMEM((tpn, seq // tpn, queries.shape[1]), bf16),
            pltpu.VMEM((tpn, seq // tpn, queries.shape[1]), bf16),
            pltpu.VMEM((2 * top * own_rows, 2 * n * cap), bf16),
            pltpu.VMEM((half, 2) + chunk, bf16),
            pltpu.VMEM((half,) + chunk, bf16),
            pltpu.VMEM((n, tpn) + chunk, bf16),
            pltpu.VMEM((n, tpn) + chunk, bf16),
            pltpu.VMEM((n, 2) + chunk, bf16),
            pltpu.VMEM((n,) + chunk, bf16),
            pltpu.VMEM((n,) + chunk, bf16),
            pltpu.VMEM((n,) + chunk, bf16),
            pltpu.VMEM((n,) + chunk, bf16),
            dma((12 + tpn,)),
            dma((n,)),
            dma((n,)),
            dma((7,)),
            dma((n,)),
            dma((half,)),
            dma((n,)),
            dma((n,)),
            dma((n,)),
            dma((2,)),
        ],
        compiler_params=pltpu.CompilerParams(
            collective_id=0, has_side_effects=True, vmem_limit_bytes=60 * 1024 * 1024
        ),
    )(
        queries,
        cum_gate,
        norm_gain.reshape(width // 128, 128),
        routes.T,
        route_weight.T,
        key_cache,
        value_cache,
        out_weight,
        routed_input,
        expert_gate,
        expert_up,
        expert_down,
    )
    return write_out(mixed, out)


def write_kernel(a, b, a_out, b_out, sem):
    copies = [
        pltpu.make_async_copy(a, a_out, sem.at[0]),
        pltpu.make_async_copy(b, b_out, sem.at[1]),
    ]
    for copy in copies:
        copy.start()
    for copy in copies:
        copy.wait()


def write_out(*arrays):
    return pl.pallas_call(
        write_kernel,
        out_shape=[jax.ShapeDtypeStruct(a.shape, a.dtype) for a in arrays],
        in_specs=[pl.BlockSpec(memory_space=pltpu.VMEM)] * len(arrays),
        out_specs=[pl.BlockSpec(memory_space=pltpu.HBM)] * len(arrays),
        scratch_shapes=[pltpu.SemaphoreType.DMA((len(arrays),))],
    )(*[pltpu.with_memory_space_constraint(a, pltpu.VMEM) for a in arrays])


def block_capacity(own_rows, top_count, expert_count):
    return max(2, own_rows * top_count * 3 // (2 * expert_count))


def slot_chooser(route_rows, expert_count, capacity):
    token_rows, top_count = route_rows.shape
    flat = route_rows.reshape(token_rows * top_count)
    same = (flat[:, None] == jnp.arange(expert_count, dtype=jnp.int32)[None, :]).astype(jnp.int32)
    earlier = jnp.cumsum(same, axis=0) - same
    rank = jnp.sum(earlier * same, axis=1)
    slot = flat * capacity + rank
    chosen = slot[:, None] == jnp.arange(expert_count * capacity, dtype=jnp.int32)[None, :]
    return chosen.astype(jnp.bfloat16).reshape(token_rows, top_count, expert_count * capacity)


def rms_rows(source, norm_gain):
    widened = source.astype(jnp.float32)
    scale = lax.rsqrt(jnp.mean(widened * widened, axis=-1, keepdims=True) + 1e-06)
    return (widened * scale * norm_gain.astype(jnp.float32)).astype(jnp.bfloat16)


def mixer_half(queries, key_cache, value_cache, cum_gate, out_weight):
    seq_rows = queries.shape[0]
    local_heads = key_cache.shape[0]
    head_size = key_cache.shape[1]
    group = queries.shape[1] // (local_heads * head_size)
    own_start = lax.axis_index("ep") * seq_rows
    query_heads = queries.reshape(seq_rows, local_heads, group, head_size)
    query_pos = own_start + jnp.arange(seq_rows, dtype=jnp.int32)
    gate_query = lax.dynamic_slice_in_dim(cum_gate, own_start, seq_rows, 1)
    gate_rows = jnp.transpose(gate_query)[:, :, None, None]
    scale = head_size ** (-0.5)
    best_start = jnp.full((seq_rows, local_heads, group), -jnp.inf, jnp.float32)
    total_start = jnp.zeros((seq_rows, local_heads, group), jnp.float32)
    summed_start = jnp.zeros((seq_rows, local_heads * group * head_size), jnp.float32)
    pieces = (
        lax.all_gather(key_cache, "ep", axis=2, tiled=True),
        lax.all_gather(value_cache, "ep", axis=2, tiled=True),
    )

    def update(state):
        best, total, summed = state
        key_piece, value_piece = pieces
        width = key_piece.shape[2]
        scores = (
            jnp.einsum("thgd,hds->thgs", query_heads, key_piece, preferred_element_type=jnp.float32)
            * scale
        )
        scores = scores + gate_rows - cum_gate[None, :, None, :]
        key_pos = jnp.arange(width, dtype=jnp.int32)
        allowed = key_pos[None, :] <= query_pos[:, None]
        scores = jnp.where(allowed[:, None, None, :], scores, -jnp.inf)
        new_best = jnp.max(scores, axis=-1)
        factor = jnp.exp(best - new_best)
        weights = jnp.exp(scores - new_best[..., None])
        new_total = total * factor + jnp.sum(weights, axis=-1)
        product = jnp.einsum(
            "thgs,hds->thgd",
            weights.astype(jnp.bfloat16),
            value_piece,
            preferred_element_type=jnp.float32,
        )
        new_summed = summed.reshape(product.shape) * factor[..., None] + product
        return (new_best, new_total, new_summed.reshape(seq_rows, local_heads * group * head_size))

    best, total, summed = lax.cond(
        jnp.int32(0) <= own_start,
        update,
        lambda state: state,
        (best_start, total_start, summed_start),
    )
    attended = summed.reshape(seq_rows, local_heads, group, head_size) / total[..., None]
    attended = attended.astype(jnp.bfloat16).reshape(seq_rows, local_heads * group * head_size)
    by_position = lax.all_to_all(attended, "tp", split_axis=0, concat_axis=1, tiled=True)
    return jnp.dot(by_position, out_weight, preferred_element_type=jnp.float32).astype(jnp.bfloat16)


def expert_half(routed_input, norm_gain, routes, route_weight, expert_gate, expert_up, expert_down):
    group_size = lax.axis_size("tp")
    ep_size = lax.axis_size("ep")
    tp_index = lax.axis_index("tp")
    seq_rows, width = routed_input.shape
    own_rows = seq_rows // group_size
    local_experts = expert_gate.shape[0]
    expert_count = local_experts * ep_size
    top_count = routes.shape[1]
    capacity = max(2, own_rows * top_count * 3 // (2 * expert_count))
    per_device = local_experts * capacity
    mine = lax.dynamic_slice_in_dim(routed_input, tp_index * own_rows, own_rows, 0)
    own_routes = lax.dynamic_slice_in_dim(routes, tp_index * own_rows, own_rows, 0)
    chooser = slot_chooser(own_routes, expert_count, capacity)
    normed = rms_rows(mine, norm_gain)
    outgoing = jnp.einsum("tks,td->sd", chooser, normed, preferred_element_type=jnp.float32).astype(
        jnp.bfloat16
    )
    arrived = lax.all_to_all(
        outgoing.reshape(1, ep_size, per_device, width),
        "ep",
        split_axis=1,
        concat_axis=1,
        tiled=True,
    )
    received = lax.all_gather(arrived, "tp", axis=0, tiled=True)
    blocks = received.shape[0]
    divide_point = received.reshape(blocks, ep_size, local_experts, capacity, width)
    gate = jnp.einsum(
        "abecd,edf->abecf", divide_point, expert_gate, preferred_element_type=jnp.float32
    )
    upper = jnp.einsum(
        "abecd,edf->abecf", divide_point, expert_up, preferred_element_type=jnp.float32
    )
    hidden = (jax.nn.silu(gate) * upper).astype(jnp.bfloat16)
    partial_value = jnp.einsum(
        "abecf,efd->abecd", hidden, expert_down, preferred_element_type=jnp.float32
    )
    rounded = lax.optimization_barrier(partial_value.astype(jnp.bfloat16)).astype(jnp.float32)
    summed = lax.psum_scatter(
        rounded.reshape(lax.axis_size("tp") * 1, ep_size, per_device, width).astype(jnp.bfloat16),
        "tp",
        scatter_dimension=0,
        tiled=True,
    )
    returned = lax.all_to_all(summed, "ep", split_axis=1, concat_axis=1, tiled=True)
    picked = jnp.einsum(
        "tks,sd->tkd",
        chooser,
        returned.reshape(ep_size * per_device, width),
        preferred_element_type=jnp.float32,
    )
    own_weight = lax.dynamic_slice_in_dim(route_weight, tp_index * own_rows, own_rows, 0)
    return jnp.sum(own_weight[:, :, None] * picked, axis=1).astype(jnp.bfloat16)


def body(
    queries,
    key_cache,
    value_cache,
    cum_gate,
    out_weight,
    routed_input,
    norm_gain,
    routes,
    route_weight,
    expert_gate,
    expert_up,
    expert_down,
):
    mixed_out = mixer_half(queries, key_cache, value_cache, cum_gate, out_weight)
    expert_out = expert_half(
        routed_input, norm_gain, routes, route_weight, expert_gate, expert_up, expert_down
    )
    return (mixed_out, expert_out)


def pick_body(
    n,
    tpn,
    queries,
    key_cache,
    value_cache,
    cum_gate,
    out_weight,
    routed_input,
    norm_gain,
    routes,
    route_weight,
    expert_gate,
    *rest,
):
    seq, columns = queries.shape
    own_rows = routed_input.shape[0] // tpn
    cap = block_capacity(own_rows, routes.shape[1], n * expert_gate.shape[0])
    fits = (
        tpn == 4
        and n == 8
        and cap % 8 == 0
        and expert_gate.shape[0] == 1
        and key_cache.shape[0] == 1
        and seq % 128 == 0
    )
    args = (
        queries,
        key_cache,
        value_cache,
        cum_gate,
        out_weight,
        routed_input,
        norm_gain,
        routes,
        route_weight,
        expert_gate,
    ) + rest
    return fused_body(n, tpn, *args) if fits else body(*args)


def solution(mesh):
    return jax.shard_map(
        functools.partial(pick_body, mesh.shape["ep"], mesh.shape["tp"]),
        mesh=mesh,
        in_specs=(
            P("ep", "tp"),
            P("tp", None, "ep"),
            P("tp", None, "ep"),
            P("tp", None),
            P(),
            P("ep", None),
            P(),
            P("ep", None),
            P("ep", None),
            P("ep", None, "tp"),
            P("ep", None, "tp"),
            P("ep", "tp", None),
        ),
        out_specs=(P(("ep", "tp"), None), P(("ep", "tp"), None)),
        check_vma=False,
    )
```

```python
import functools

import jax
import jax.numpy as jnp
from jax import lax
from jax.experimental import pallas as pl
from jax.experimental.pallas import tpu as pltpu
from jax.sharding import PartitionSpec as P

MESH = pl.DeviceIdType.MESH


INNER_SENDS = (1, 2, 3, 6, 5, 7, 4)
OUTER_SENDS = (4, 2, 7, 5, 1, 6, 3)
INNER_STEPS = (
    "C0", "D0", "A6", "E0", "B6", "A2", "A5", "C2", "D2", "A7", "C6", "B5", "D6", "C5",
    "D5", "E2", "B7", "C7", "E6", "A1", "A4", "A3", "C3", "E5", "D7", "C1", "D1", "B4",
    "K", "D3", "C4", "E7", "D4", "E1", "E3", "E4", "T",
)
OUTER_STEPS = (
    "C0", "D0", "A4", "A1", "E0", "C1", "D1", "B4", "A7", "C4", "D4", "E1", "A6", "A2",
    "B7", "E4", "A5", "C7", "A3", "C2", "D7", "B6", "C3", "D3", "K", "C6", "B5", "E7",
    "D6", "C5", "E3", "D5", "E6", "D2", "T", "E5", "E2",
)


def fused_kernel(
    n,
    tpn,
    cap,
    q_any,
    gate_any,
    gain_any,
    routes_any,
    rw_any,
    k_any,
    v_any,
    ow_any,
    x_any,
    wg_any,
    wu_any,
    wd_any,
    mixed_ref,
    out_ref,
    q_ref,
    gate_ref,
    gain_ref,
    routes_ref,
    rw_ref,
    xbuf,
    wgv,
    wuv,
    wdv,
    owv,
    kv,
    att,
    attr,
    sel,
    sbuf,
    sfar,
    recv,
    part,
    r1,
    s2,
    r2,
    s3,
    rbuf,
    lsem,
    kvs,
    kvr,
    sent,
    a_r,
    bx_r,
    f_r,
    r1_r,
    r2_r,
    all_r,
):
    e = lax.axis_index("ep")
    t = lax.axis_index("tp")
    partner = t + 1 - 2 * lax.rem(t, 2)
    peer = lax.rem(t + 2, tpn)
    opp = lax.rem(partner + 2, tpn)
    mate = e + 1 - 2 * lax.rem(e, 2)
    half = n // 2
    _, own_rows, width = xbuf.shape
    wide = width // 2
    head = k_any.shape[1]
    seq = q_ref.shape[0]

    side = lax.div(e, half)
    base = side * half
    local = lax.rem(e, half)
    row = lax.rem(e, 2)
    inner = lax.div(local, 2) == 1 - side
    rank = jnp.where(inner, 0, 1)

    barrier = pltpu.get_barrier_semaphore()
    for s in range(1, n):
        pl.semaphore_signal(
            barrier, inc=1, device_id={"ep": lax.rem(e + s, n), "tp": t}, device_id_type=MESH
        )
    for s in range(1, tpn):
        pl.semaphore_signal(
            barrier, inc=1, device_id={"ep": e, "tp": lax.rem(t + s, tpn)}, device_id_type=MESH
        )

    blocks = (t, peer, partner, opp)

    def load_x(j):
        at = blocks[j] * own_rows
        return pltpu.make_async_copy(x_any.at[pl.ds(at, own_rows)], xbuf.at[j], lsem.at[11 + j])

    load_k = pltpu.make_async_copy(k_any.at[0], kv.at[e, pl.ds(0, head)], lsem.at[1])
    load_v = pltpu.make_async_copy(v_any.at[0], kv.at[e, pl.ds(head, head)], lsem.at[2])
    load_g = pltpu.make_async_copy(wg_any.at[0], wgv, lsem.at[3])
    load_u = pltpu.make_async_copy(wu_any.at[0], wuv, lsem.at[4])
    load_d = pltpu.make_async_copy(wd_any.at[0], wdv, lsem.at[5])
    load_o = pltpu.make_async_copy(ow_any, owv, lsem.at[6])
    load_q = pltpu.make_async_copy(q_any, q_ref, lsem.at[8])
    load_c = pltpu.make_async_copy(gate_any, gate_ref, lsem.at[9])
    load_n = pltpu.make_async_copy(gain_any, gain_ref, lsem.at[10])
    load_r = pltpu.make_async_copy(routes_any, routes_ref, lsem.at[7])
    load_w = pltpu.make_async_copy(rw_any, rw_ref, lsem.at[0])
    load_r.start()
    load_n.start()
    load_x(0).start()
    load_x(1).start()
    load_k.start()
    load_v.start()
    for j in range(2, tpn):
        load_x(j).start()
    load_g.start()
    load_u.start()
    load_d.start()
    load_w.start()
    load_q.start()
    load_c.start()
    load_o.start()

    def remote(src, dst, ssem, rsem, ep, tp):
        return pltpu.make_async_remote_copy(
            src_ref=src,
            dst_ref=dst,
            send_sem=ssem,
            recv_sem=rsem,
            device_id={"ep": ep, "tp": tp},
            device_id_type=MESH,
        )

    def flip(s):
        s = jnp.int32(s)
        flipped = jnp.int32(0)
        bit = 1
        while bit < n:
            ours = lax.rem(lax.div(e, jnp.int32(bit)), jnp.int32(2))
            theirs = lax.rem(lax.div(s, jnp.int32(bit)), jnp.int32(2))
            flipped = flipped + bit * (ours + theirs - 2 * ours * theirs)
            bit *= 2
        return flipped

    def kv_far(s):
        return remote(kv.at[e], kv.at[e], kvs.at[s - 1], kvr.at[s - 1], lax.rem(e + 2 * s, n), t)

    def kv_far_in(s):
        src = lax.rem(e - 2 * s + n, n)
        return remote(kv.at[src], kv.at[src], kvs.at[s - 1], kvr.at[s - 1], lax.rem(e + 2 * s, n), t)

    def kv_mate(s):
        src = lax.rem(e - 2 * s + n, n)
        return remote(kv.at[src], kv.at[src], kvs.at[half - 1 + s], kvr.at[half - 1 + s], mate, t)

    def kv_mate_in(s):
        src = lax.rem(mate - 2 * s + n, n)
        return remote(kv.at[src], kv.at[src], kvs.at[half - 1 + s], kvr.at[half - 1 + s], mate, t)

    def far_sends(s):
        return e + 2 * s < n

    def far_comes(s):
        return e - 2 * s >= 0

    def mate_sends(s):
        return (e - 2 * s >= 0) if s else row == 0

    def mate_comes(s):
        return (mate - 2 * s >= 0) if s else row == 1

    def near(s):
        dst = flip(s)
        return remote(
            sbuf.at[lax.rem(dst, half)],
            recv.at[s, pl.ds(0, 2)],
            sent.at[0],
            a_r.at[s - 1],
            dst,
            t,
        )

    def far(g):
        dst = source(g)
        mine = half + 2 * rank + g % 2
        return remote(
            sfar.at[lax.rem(dst, half)], recv.at[mine, 0], sent.at[0], a_r.at[mine - 1], dst, t
        )

    def arrival(g):
        if g < half:
            return remote(sbuf.at[0], recv.at[g, pl.ds(0, 2)], sent.at[0], a_r.at[g - 1], e, peer)
        return remote(sfar.at[0], recv.at[g, 0], sent.at[0], a_r.at[g - 1], e, peer)

    def copy_bx(g):
        return remote(recv.at[g, 0], recv.at[g, 1], sent.at[1], bx_r.at[g - half], e, peer)

    def copy_f(g):
        return remote(
            recv.at[g, pl.ds(0, 2)], recv.at[g, pl.ds(2, 2)], sent.at[2], f_r.at[g - 1], e, partner
        )

    def copy_r1(g):
        return remote(part.at[g, pl.ds(2, 2)], r1.at[g], sent.at[3], r1_r.at[g], e, partner)

    def copy_r2(g):
        return remote(s2.at[g], r2.at[g], sent.at[4], r2_r.at[g], e, peer)

    def source(g):
        g = jnp.int32(g)
        which = lax.div(g - half, jnp.int32(2))
        turn = lax.rem(g, jnp.int32(2))
        z = jnp.where(side == 0, 2 + which, 1 - which)
        far = 2 * z + row + turn - 2 * row * turn
        return jnp.where(g < half, flip(g), far)

    def copy_r3(g):
        return remote(s3.at[g], rbuf.at[e], sent.at[5], all_r.at[0], source(g), t)

    top, share = routes_ref.shape

    def column(line, block):
        at = block * own_rows
        own = lax.broadcasted_iota(jnp.int32, (own_rows, share), 1) == (
            lax.broadcasted_iota(jnp.int32, (own_rows, share), 0) + at
        )
        return jnp.sum(
            jnp.where(own, jnp.broadcast_to(line, own.shape), 0.0), axis=1, keepdims=True
        )

    def named_by(ref, block):
        return [column(ref[k : k + 1, :].astype(jnp.float32), block) for k in range(top)]

    before = lax.broadcasted_iota(jnp.int32, (own_rows, own_rows), 1) < lax.broadcasted_iota(
        jnp.int32, (own_rows, own_rows), 0
    )

    def lanes_of(first, count):
        lanes = 2 * count * cap
        place = lax.broadcasted_iota(jnp.int32, (own_rows, lanes), 1).astype(jnp.float32) + 0.5
        expert = jnp.floor(place / (2.0 * cap))
        inside = place - 0.5 - expert * (2.0 * cap)
        right = inside >= cap
        slot = jnp.where(right, inside - cap, inside)
        return expert + first.astype(jnp.float32), right, slot

    def hits_of(names, lanes):
        expert, right, slot = lanes
        named = [name == expert for name in names]
        total = sum([m.astype(jnp.float32) for m in named])
        ranks = jnp.dot(
            before.astype(jnp.bfloat16),
            total.astype(jnp.bfloat16),
            preferred_element_type=jnp.float32,
        )
        return named, total, ranks == slot

    def spread_of(names, lanes):
        _, total, hit = hits_of(names, lanes)
        right = lanes[1]
        chosen = jnp.where(hit, total, 0.0)
        spread = jnp.concatenate(
            [jnp.where(right, 0.0, chosen), jnp.where(right, chosen, 0.0)], axis=0
        )
        return spread.T.astype(jnp.bfloat16)

    def chunks(spread, rows):
        return jnp.dot(spread, rows, preferred_element_type=jnp.float32).astype(jnp.bfloat16)

    with jax.named_scope("w_r"):
        load_r.wait()
    side_lanes = lanes_of(base, half)
    own_names = named_by(routes_ref, t)
    spread = spread_of(own_names, side_lanes)
    load_n.wait()
    gain = gain_ref[...].astype(jnp.float32)
    gain = jnp.concatenate([gain[j : j + 1, :] for j in range(gain.shape[0])], axis=1)

    def halves(j):
        with jax.named_scope(f"w_x{j}"):
            load_x(j).wait()
        x = xbuf[j].astype(jnp.float32)
        scale = lax.rsqrt(jnp.mean(x * x, axis=-1, keepdims=True) + 1e-06)
        normed = (x * scale * gain).astype(jnp.bfloat16)
        return jnp.concatenate([normed[:, :wide], normed[:, wide:]], axis=0)

    own = halves(0)
    sbuf[:, 0] = chunks(spread, own).reshape(half, 2 * cap, wide)
    sfar[...] = chunks(spread_of(own_names, lanes_of(half - base, half)), own).reshape(sfar.shape)

    sbuf[:, 1] = chunks(spread_of(named_by(routes_ref, peer), side_lanes), halves(1)).reshape(
        half, 2 * cap, wide
    )

    with jax.named_scope("barrier"):
        pl.semaphore_wait(barrier, n - 1 + tpn - 1)

    def send(which):
        for g in which:
            (near if g < half else far)(g).start()

    def by_place(inner_part, outer_part):
        @pl.when(inner)
        def _():
            send(inner_part)

        @pl.when(jnp.logical_not(inner))
        def _():
            send(outer_part)

    by_place(INNER_SENDS, OUTER_SENDS)
    load_k.wait()
    load_v.wait()
    for s in range(1, half):

        @pl.when(far_sends(s))
        def _():
            kv_far(s).start()

    @pl.when(mate_sends(0))
    def _():
        kv_mate(0).start()

    own_lanes = lanes_of(e, 1)
    recv[0, 0:2] = sbuf[local]
    for j in (2, 3):
        recv[0, j] = chunks(spread_of(named_by(routes_ref, blocks[j]), own_lanes), halves(j))

    def copy_att(s):
        dst = lax.rem(t + s, tpn)
        return remote(att.at[dst], attr.at[t], sent.at[6], all_r.at[1], e, dst)

    def joint(ref, ssem, rsem):
        return remote(ref, ref, ssem, rsem, e, peer)

    att_joint = joint(attr.at[pl.ds(0, tpn - 1)], sent.at[6], all_r.at[1])

    def attention():
        for s in range(half):

            @pl.when(mate_comes(s))
            def _():
                kv_mate_in(s).wait_recv()

        for j in range(1, n):

            @pl.when(j > e)
            def _():
                kv[j] = jnp.zeros(kv.shape[1:], kv.dtype)

        load_q.wait()
        load_c.wait()
        own_gate = gate_ref[:, pl.ds(pl.multiple_of(e * seq, seq), seq)]
        eye = lax.broadcasted_iota(jnp.int32, (seq, seq), 0) == lax.broadcasted_iota(
            jnp.int32, (seq, seq), 1
        )
        gate_col = jnp.sum(
            jnp.where(eye, jnp.broadcast_to(own_gate, (seq, seq)), 0.0), axis=1, keepdims=True
        )
        key_pos = lax.broadcasted_iota(jnp.int32, (seq, n * seq), 1)
        query_pos = lax.broadcasted_iota(jnp.int32, (seq, n * seq), 0) + e * seq
        bias = gate_col - gate_ref[...]
        group = q_ref.shape[1] // head
        heads_out = []
        for g in range(group):
            q = q_ref[:, g * head : (g + 1) * head]
            scores = jnp.concatenate(
                [
                    jnp.dot(q, kv[j, 0:head, :], preferred_element_type=jnp.float32)
                    for j in range(n)
                ],
                axis=1,
            )
            scores = scores * (head ** (-0.5)) + bias
            scores = jnp.where(key_pos <= query_pos, scores, -jnp.inf)
            weights = jnp.exp(scores - jnp.max(scores, axis=-1, keepdims=True))
            whole = jnp.sum(weights, axis=-1, keepdims=True)
            weights = weights.astype(jnp.bfloat16)
            summed = jnp.zeros((seq, head), jnp.float32)
            for j in range(n):
                summed = summed + lax.dot_general(
                    weights[:, j * seq : (j + 1) * seq],
                    kv[j, head : 2 * head, :],
                    (((1,), (1,)), ((), ())),
                    preferred_element_type=jnp.float32,
                )
            heads_out.append(summed / whole)
        attended = jnp.concatenate(heads_out, axis=1).astype(jnp.bfloat16)
        att[...] = attended.reshape(att.shape)
        attr[t] = att[t]
        for s in range(1, tpn):
            copy_att(s).start()

    def pass_kv():
        for s in range(1, half):

            @pl.when(far_comes(s))
            def _():
                kv_far_in(s).wait_recv()
                kv_mate(s).start()

    def arrive(g):
        arrival(g).wait_recv()
        (copy_f if g < half else copy_bx)(g).start()

    def spread_pair(g):
        copy_bx(g).wait_recv()
        copy_f(g).start()

    def experts(g):
        if g:
            with jax.named_scope(f"w_f{g}"):
                copy_f(g).wait_recv()
        block = recv[g].astype(jnp.float32)
        count = block.shape[0] * cap
        lo = block[:, :cap].reshape(count, wide).astype(jnp.bfloat16)
        hi = block[:, cap:].reshape(count, wide).astype(jnp.bfloat16)
        gate = jnp.dot(lo, wgv[0:wide, :], preferred_element_type=jnp.float32) + jnp.dot(
            hi, wgv[wide:, :], preferred_element_type=jnp.float32
        )
        upper = jnp.dot(lo, wuv[0:wide, :], preferred_element_type=jnp.float32) + jnp.dot(
            hi, wuv[wide:, :], preferred_element_type=jnp.float32
        )
        hidden = (gate / (1.0 + jnp.exp(-gate)) * upper).astype(jnp.bfloat16)
        down = jnp.dot(hidden, wdv[...], preferred_element_type=jnp.float32)
        shape = (tpn, cap, wide)
        part[g] = jnp.concatenate(
            [down[:, :wide].reshape(shape), down[:, wide:].reshape(shape)], axis=1
        ).astype(jnp.bfloat16)
        copy_r1(g).start()

    def cross(g):
        copy_r1(g).wait_recv()
        s2[g] = (part[g, 1].astype(jnp.float32) + r1[g, 1].astype(jnp.float32)).astype(
            jnp.bfloat16
        )
        copy_r2(g).start()

    def give_back(g):
        copy_r2(g).wait_recv()
        done = (
            part[g, 0].astype(jnp.float32)
            + r1[g, 0].astype(jnp.float32)
            + r2[g].astype(jnp.float32)
        ).astype(jnp.bfloat16)
        if g == 0:
            rbuf[e] = done
        else:
            s3[g] = done
            copy_r3(g).start()

    def first_matmul():
        load_g.wait()
        load_u.wait()
        load_d.wait()

    def choose_back():
        everywhere = lanes_of(e * 0, n)
        named, _, hit = hits_of(own_names, everywhere)
        right = everywhere[1]
        for k in range(top):
            mine = jnp.where(hit & named[k], 1.0, 0.0)
            sel[2 * k * own_rows : (2 * k + 1) * own_rows, :] = jnp.where(
                right, 0.0, mine
            ).astype(jnp.bfloat16)
            sel[(2 * k + 1) * own_rows : (2 * k + 2) * own_rows, :] = jnp.where(
                right, mine, 0.0
            ).astype(jnp.bfloat16)

    kinds = {"A": arrive, "B": spread_pair, "C": experts, "D": cross, "E": give_back}

    def run(steps):
        for name in steps:
            with jax.named_scope(name):
                if name == "K":
                    pass_kv()
                elif name == "T":
                    attention()
                else:
                    kinds[name[0]](int(name[1:]))

    first_matmul()

    @pl.when(inner)
    def _():
        run(INNER_STEPS)

    @pl.when(jnp.logical_not(inner))
    def _():
        run(OUTER_STEPS)

    choose_back()

    with jax.named_scope("w_att"):
        att_joint.wait_recv()
        load_o.wait()
    joined = jnp.concatenate([attr[j] for j in range(tpn)], axis=1)
    mixed_ref[...] = jnp.dot(joined, owv[...], preferred_element_type=jnp.float32).astype(
        jnp.bfloat16
    )
    load_w.wait()
    rw = [column(rw_ref[k : k + 1, :], t) for k in range(top)]

    fives = recv.at[pl.ds(0, half + 1), pl.ds(0, 2)]
    for which, ref in enumerate(
        (
            fives,
            recv.at[pl.ds(half, half), 0],
            recv.at[pl.ds(1, n - 1), pl.ds(0, 2)],
            part.at[:, pl.ds(2, 2)],
            s2,
        )
    ):
        joint(ref, sent.at[which], all_r.at[0]).wait_send()
    for s in range(1, half):

        @pl.when(far_sends(s))
        def _():
            kv_far(s).wait_send()

    for s in range(half):

        @pl.when(mate_sends(s))
        def _():
            kv_mate(s).wait_send()

    att_joint.wait_send()

    with jax.named_scope("w_r3"):
        joint(rbuf.at[pl.ds(0, n - 1)], sent.at[5], all_r.at[0]).wait_recv()
    lanes = 2 * n * cap
    picked = jnp.dot(
        sel[...], rbuf[...].reshape(lanes, wide), preferred_element_type=jnp.float32
    )
    for h in range(2):
        acc = jnp.zeros((own_rows, wide), jnp.float32)
        for k in range(top):
            at = (2 * k + h) * own_rows
            acc = acc + rw[k] * picked[at : at + own_rows]
        out_ref[:, h * wide : (h + 1) * wide] = acc.astype(jnp.bfloat16)

    joint(s3.at[pl.ds(1, n - 1)], sent.at[5], all_r.at[0]).wait_send()


def fused_body(
    n,
    tpn,
    queries,
    key_cache,
    value_cache,
    cum_gate,
    out_weight,
    routed_input,
    norm_gain,
    routes,
    route_weight,
    expert_gate,
    expert_up,
    expert_down,
):
    seq = queries.shape[0]
    head = key_cache.shape[1]
    width = routed_input.shape[1]
    wide = width // 2
    own_rows = routed_input.shape[0] // tpn
    top = routes.shape[1]
    units = expert_gate.shape[2]
    cap = block_capacity(own_rows, top, n * expert_gate.shape[0])
    half = n // 2
    bf16 = jnp.bfloat16
    chunk = (2 * cap, wide)
    anywhere = pl.BlockSpec(memory_space=pltpu.HBM)
    vmem = pl.BlockSpec(memory_space=pltpu.VMEM)
    dma = pltpu.SemaphoreType.DMA
    mixed, out = pl.pallas_call(
        functools.partial(fused_kernel, n, tpn, cap),
        out_shape=(
            pltpu.VMEM((seq // tpn, width), bf16),
            pltpu.VMEM((own_rows, width), bf16),
        ),
        in_specs=[anywhere] * 12,
        out_specs=(vmem, vmem),
        scratch_shapes=[
            pltpu.VMEM(queries.shape, bf16),
            pltpu.VMEM(cum_gate.shape, jnp.float32),
            pltpu.VMEM((width // 128, 128), bf16),
            pltpu.VMEM((top, tpn * own_rows), jnp.int32),
            pltpu.VMEM((top, tpn * own_rows), jnp.float32),
            pltpu.VMEM((tpn, own_rows, width), bf16),
            pltpu.VMEM((width, units), bf16),
            pltpu.VMEM((width, units), bf16),
            pltpu.VMEM((units, width), bf16),
            pltpu.VMEM(out_weight.shape, bf16),
            pltpu.VMEM((n, 2 * head, seq), bf16),
            pltpu.VMEM((tpn, seq // tpn, queries.shape[1]), bf16),
            pltpu.VMEM((tpn, seq // tpn, queries.shape[1]), bf16),
            pltpu.VMEM((2 * top * own_rows, 2 * n * cap), bf16),
            pltpu.VMEM((half, 2) + chunk, bf16),
            pltpu.VMEM((half,) + chunk, bf16),
            pltpu.VMEM((n, tpn) + chunk, bf16),
            pltpu.VMEM((n, tpn) + chunk, bf16),
            pltpu.VMEM((n, 2) + chunk, bf16),
            pltpu.VMEM((n,) + chunk, bf16),
            pltpu.VMEM((n,) + chunk, bf16),
            pltpu.VMEM((n,) + chunk, bf16),
            pltpu.VMEM((n,) + chunk, bf16),
            dma((11 + tpn,)),
            dma((n - 1,)),
            dma((n - 1,)),
            dma((7,)),
            dma((n - 1,)),
            dma((half,)),
            dma((n - 1,)),
            dma((n,)),
            dma((n,)),
            dma((2,)),
        ],
        compiler_params=pltpu.CompilerParams(
            collective_id=0, has_side_effects=True, vmem_limit_bytes=60 * 1024 * 1024
        ),
    )(
        queries,
        cum_gate,
        norm_gain.reshape(width // 128, 128),
        routes.T,
        route_weight.T,
        key_cache,
        value_cache,
        out_weight,
        routed_input,
        expert_gate,
        expert_up,
        expert_down,
    )
    return write_out(mixed, out)


def write_kernel(a, b, a_out, b_out, sem):
    copies = [
        pltpu.make_async_copy(a, a_out, sem.at[0]),
        pltpu.make_async_copy(b, b_out, sem.at[1]),
    ]
    for copy in copies:
        copy.start()
    for copy in copies:
        copy.wait()


def write_out(*arrays):
    return pl.pallas_call(
        write_kernel,
        out_shape=[jax.ShapeDtypeStruct(a.shape, a.dtype) for a in arrays],
        in_specs=[pl.BlockSpec(memory_space=pltpu.VMEM)] * len(arrays),
        out_specs=[pl.BlockSpec(memory_space=pltpu.HBM)] * len(arrays),
        scratch_shapes=[pltpu.SemaphoreType.DMA((len(arrays),))],
    )(*[pltpu.with_memory_space_constraint(a, pltpu.VMEM) for a in arrays])


def block_capacity(own_rows, top_count, expert_count):
    return max(2, own_rows * top_count * 3 // (2 * expert_count))


def slot_chooser(route_rows, expert_count, capacity):
    token_rows, top_count = route_rows.shape
    flat = route_rows.reshape(token_rows * top_count)
    same = (flat[:, None] == jnp.arange(expert_count, dtype=jnp.int32)[None, :]).astype(jnp.int32)
    earlier = jnp.cumsum(same, axis=0) - same
    rank = jnp.sum(earlier * same, axis=1)
    slot = flat * capacity + rank
    chosen = slot[:, None] == jnp.arange(expert_count * capacity, dtype=jnp.int32)[None, :]
    return chosen.astype(jnp.bfloat16).reshape(token_rows, top_count, expert_count * capacity)


def rms_rows(source, norm_gain):
    widened = source.astype(jnp.float32)
    scale = lax.rsqrt(jnp.mean(widened * widened, axis=-1, keepdims=True) + 1e-06)
    return (widened * scale * norm_gain.astype(jnp.float32)).astype(jnp.bfloat16)


def mixer_half(queries, key_cache, value_cache, cum_gate, out_weight):
    seq_rows = queries.shape[0]
    local_heads = key_cache.shape[0]
    head_size = key_cache.shape[1]
    group = queries.shape[1] // (local_heads * head_size)
    own_start = lax.axis_index("ep") * seq_rows
    query_heads = queries.reshape(seq_rows, local_heads, group, head_size)
    query_pos = own_start + jnp.arange(seq_rows, dtype=jnp.int32)
    gate_query = lax.dynamic_slice_in_dim(cum_gate, own_start, seq_rows, 1)
    gate_rows = jnp.transpose(gate_query)[:, :, None, None]
    scale = head_size ** (-0.5)
    best_start = jnp.full((seq_rows, local_heads, group), -jnp.inf, jnp.float32)
    total_start = jnp.zeros((seq_rows, local_heads, group), jnp.float32)
    summed_start = jnp.zeros((seq_rows, local_heads * group * head_size), jnp.float32)
    pieces = (
        lax.all_gather(key_cache, "ep", axis=2, tiled=True),
        lax.all_gather(value_cache, "ep", axis=2, tiled=True),
    )

    def update(state):
        best, total, summed = state
        key_piece, value_piece = pieces
        width = key_piece.shape[2]
        scores = (
            jnp.einsum("thgd,hds->thgs", query_heads, key_piece, preferred_element_type=jnp.float32)
            * scale
        )
        scores = scores + gate_rows - cum_gate[None, :, None, :]
        key_pos = jnp.arange(width, dtype=jnp.int32)
        allowed = key_pos[None, :] <= query_pos[:, None]
        scores = jnp.where(allowed[:, None, None, :], scores, -jnp.inf)
        new_best = jnp.max(scores, axis=-1)
        factor = jnp.exp(best - new_best)
        weights = jnp.exp(scores - new_best[..., None])
        new_total = total * factor + jnp.sum(weights, axis=-1)
        product = jnp.einsum(
            "thgs,hds->thgd",
            weights.astype(jnp.bfloat16),
            value_piece,
            preferred_element_type=jnp.float32,
        )
        new_summed = summed.reshape(product.shape) * factor[..., None] + product
        return (new_best, new_total, new_summed.reshape(seq_rows, local_heads * group * head_size))

    best, total, summed = lax.cond(
        jnp.int32(0) <= own_start,
        update,
        lambda state: state,
        (best_start, total_start, summed_start),
    )
    attended = summed.reshape(seq_rows, local_heads, group, head_size) / total[..., None]
    attended = attended.astype(jnp.bfloat16).reshape(seq_rows, local_heads * group * head_size)
    by_position = lax.all_to_all(attended, "tp", split_axis=0, concat_axis=1, tiled=True)
    return jnp.dot(by_position, out_weight, preferred_element_type=jnp.float32).astype(jnp.bfloat16)


def expert_half(routed_input, norm_gain, routes, route_weight, expert_gate, expert_up, expert_down):
    group_size = lax.axis_size("tp")
    ep_size = lax.axis_size("ep")
    tp_index = lax.axis_index("tp")
    seq_rows, width = routed_input.shape
    own_rows = seq_rows // group_size
    local_experts = expert_gate.shape[0]
    expert_count = local_experts * ep_size
    top_count = routes.shape[1]
    capacity = max(2, own_rows * top_count * 3 // (2 * expert_count))
    per_device = local_experts * capacity
    mine = lax.dynamic_slice_in_dim(routed_input, tp_index * own_rows, own_rows, 0)
    own_routes = lax.dynamic_slice_in_dim(routes, tp_index * own_rows, own_rows, 0)
    chooser = slot_chooser(own_routes, expert_count, capacity)
    normed = rms_rows(mine, norm_gain)
    outgoing = jnp.einsum("tks,td->sd", chooser, normed, preferred_element_type=jnp.float32).astype(
        jnp.bfloat16
    )
    arrived = lax.all_to_all(
        outgoing.reshape(1, ep_size, per_device, width),
        "ep",
        split_axis=1,
        concat_axis=1,
        tiled=True,
    )
    received = lax.all_gather(arrived, "tp", axis=0, tiled=True)
    blocks = received.shape[0]
    divide_point = received.reshape(blocks, ep_size, local_experts, capacity, width)
    gate = jnp.einsum(
        "abecd,edf->abecf", divide_point, expert_gate, preferred_element_type=jnp.float32
    )
    upper = jnp.einsum(
        "abecd,edf->abecf", divide_point, expert_up, preferred_element_type=jnp.float32
    )
    hidden = (jax.nn.silu(gate) * upper).astype(jnp.bfloat16)
    partial_value = jnp.einsum(
        "abecf,efd->abecd", hidden, expert_down, preferred_element_type=jnp.float32
    )
    rounded = lax.optimization_barrier(partial_value.astype(jnp.bfloat16)).astype(jnp.float32)
    summed = lax.psum_scatter(
        rounded.reshape(lax.axis_size("tp") * 1, ep_size, per_device, width).astype(jnp.bfloat16),
        "tp",
        scatter_dimension=0,
        tiled=True,
    )
    returned = lax.all_to_all(summed, "ep", split_axis=1, concat_axis=1, tiled=True)
    picked = jnp.einsum(
        "tks,sd->tkd",
        chooser,
        returned.reshape(ep_size * per_device, width),
        preferred_element_type=jnp.float32,
    )
    own_weight = lax.dynamic_slice_in_dim(route_weight, tp_index * own_rows, own_rows, 0)
    return jnp.sum(own_weight[:, :, None] * picked, axis=1).astype(jnp.bfloat16)


def body(
    queries,
    key_cache,
    value_cache,
    cum_gate,
    out_weight,
    routed_input,
    norm_gain,
    routes,
    route_weight,
    expert_gate,
    expert_up,
    expert_down,
):
    mixed_out = mixer_half(queries, key_cache, value_cache, cum_gate, out_weight)
    expert_out = expert_half(
        routed_input, norm_gain, routes, route_weight, expert_gate, expert_up, expert_down
    )
    return (mixed_out, expert_out)


def pick_body(
    n,
    tpn,
    queries,
    key_cache,
    value_cache,
    cum_gate,
    out_weight,
    routed_input,
    norm_gain,
    routes,
    route_weight,
    expert_gate,
    *rest,
):
    seq, columns = queries.shape
    own_rows = routed_input.shape[0] // tpn
    cap = block_capacity(own_rows, routes.shape[1], n * expert_gate.shape[0])
    fits = (
        tpn == 4
        and n == 8
        and cap % 8 == 0
        and expert_gate.shape[0] == 1
        and key_cache.shape[0] == 1
        and seq % 128 == 0
    )
    args = (
        queries,
        key_cache,
        value_cache,
        cum_gate,
        out_weight,
        routed_input,
        norm_gain,
        routes,
        route_weight,
        expert_gate,
    ) + rest
    return fused_body(n, tpn, *args) if fits else body(*args)


def solution(mesh):
    return jax.shard_map(
        functools.partial(pick_body, mesh.shape["ep"], mesh.shape["tp"]),
        mesh=mesh,
        in_specs=(
            P("ep", "tp"),
            P("tp", None, "ep"),
            P("tp", None, "ep"),
            P("tp", None),
            P(),
            P("ep", None),
            P(),
            P("ep", None),
            P("ep", None),
            P("ep", None, "tp"),
            P("ep", None, "tp"),
            P("ep", "tp", None),
        ),
        out_specs=(P(("ep", "tp"), None), P(("ep", "tp"), None)),
        check_vma=False,
    )
```
